32 devices in a mesh: sp: 16 (over z, y, x), tp: 2 (over core).
Axes of the slice: x: 2, y: 2, z: 4, core: 2. Of those that a mesh axis runs over, the one named last changes fastest.
Arguments:
- queries: bfloat16 [4096, 1024], P('sp', 'tp'), may hold values from -12 to 12
- keys: bfloat16 [4096, 1024], P('sp', 'tp'), may hold values from -6 to 6
- values: bfloat16 [4096, 1024], P('sp', 'tp'), may hold values from -6 to 6
- w_out: bfloat16 [1024, 2048], P(None, 'tp'), may hold values from -0.375 to 0.375
Outputs:
- mixed: bfloat16 [4096, 2048], P('sp', 'tp')
The draws below stay inside these ranges and needn't reach their ends.
All inputs are finite; a program needn't handle non-finite values.
Results may differ from the reference program's by a relative error of at most 0.0056.
Values may be sent and summed in bfloat16 or wider, within the bound.
No kernel may reach another device: no remote copies, remote signals or barrier semaphores. Data moves between devices by JAX's collectives and lax.ppermute only.
A program may use at most 64 MiB of HBM per device.

```python
import math
import jax
import jax.numpy as jnp
from jax import lax

HEADS = 8
HEAD_DIM = 128
D = 2048
SIDE_KEY_COUNT = 64
MIDDLE_DILATION = 4
FAR_DILATION = 16
TOKENS = 4096


def draw_queries(key, part):
    shape = (TOKENS, HEADS * HEAD_DIM)
    drawn = jnp.clip(2.0 * jax.random.normal(jax.random.fold_in(key, 1), shape, jnp.float32), -12.0, 12.0)
    return drawn.astype(jnp.bfloat16)


def draw_keys(key, part):
    shape = (TOKENS, HEADS * HEAD_DIM)
    drawn = jnp.clip(jax.random.normal(jax.random.fold_in(key, 2), shape, jnp.float32), -6.0, 6.0)
    return drawn.astype(jnp.bfloat16)


def levels(own_key, shape, split, least, largest):
    def one(dim, blocks):
        draws = jax.random.uniform(jax.random.fold_in(jax.random.fold_in(own_key, 6), dim), (blocks,), jnp.float32, least / len(split), largest / len(split))
        return jnp.repeat(jnp.exp(draws), shape[dim] // blocks).reshape((-1,) + (1,) * (len(shape) - dim - 1))

    loudness = one(*split[0])
    for cut in split[1:]:
        loudness = loudness * one(*cut)
    return loudness


def gaussian(own_key, shape, width, bound, cuts=(), kind=jnp.bfloat16):
    level = levels(own_key, shape, cuts, -0.22, 0.18) if cuts else 1.0
    values = jax.random.normal(own_key, shape, jnp.float32) * width * level
    return jnp.minimum(jnp.maximum(values, -bound), bound).astype(kind)


def setup_inputs(seed: int = 0) -> dict:
    key_of = jax.random.split(jax.random.key(seed), 5)
    queries = draw_queries(jax.random.fold_in(key_of[4], 71), 0)
    keys = draw_keys(jax.random.fold_in(key_of[4], 71), 0)
    values = gaussian(key_of[2], (TOKENS, HEADS * HEAD_DIM), 1.0, 6.0, ((0, 16), (1, 2)))
    w_out = gaussian(key_of[3], (HEADS * HEAD_DIM, D), (HEADS * HEAD_DIM // 4) ** -0.5, 0.375, ((1, 2),))
    return dict(queries=queries, keys=keys, values=values, w_out=w_out)


def block_rows(count):
    return count if count <= 128 else math.gcd(count, 128)


def band_scores(queries, keys, values, dilation_step):
    sequence_length, columns = queries.shape
    heads = columns // HEAD_DIM
    residue_rows = sequence_length // dilation_step
    rows_block = block_rows(residue_rows)
    blocks = residue_rows // rows_block
    span = rows_block + 2 * SIDE_KEY_COUNT
    padding = SIDE_KEY_COUNT * dilation_step
    padded_keys = jnp.pad(keys, ((padding, padding), (0, 0))).reshape(residue_rows + 2 * SIDE_KEY_COUNT, dilation_step, heads, HEAD_DIM)
    padded_values = jnp.pad(values, ((padding, padding), (0, 0))).reshape(residue_rows + 2 * SIDE_KEY_COUNT, dilation_step, heads, HEAD_DIM)
    grouped = queries.reshape(blocks, rows_block, dilation_step, heads, HEAD_DIM)
    query_idx = jnp.arange(rows_block, dtype=jnp.int32)[:, None]
    key_idx = jnp.arange(span, dtype=jnp.int32)[None, :]
    in_band = (key_idx >= query_idx) & (key_idx <= query_idx + 2 * SIDE_KEY_COUNT)
    residues = jnp.arange(dilation_step, dtype=jnp.int32)[:, None, None, None]
    scale = HEAD_DIM ** -0.5

    def one_block(inputs):
        number, query_block = inputs
        first_row = (number * rows_block).astype(jnp.int32)
        key_window = lax.dynamic_slice_in_dim(padded_keys, first_row, span, 0)
        value_window = lax.dynamic_slice_in_dim(padded_values, first_row, span, 0)
        scores = jnp.einsum('qrhe,krhe->rhqk', query_block.astype(jnp.float32), key_window.astype(jnp.float32)) * scale
        key_pos = (first_row + key_idx[None, None] - SIDE_KEY_COUNT) * dilation_step + residues
        allowed = in_band[None, None] & (key_pos >= 0) & (key_pos < sequence_length)
        scores = jnp.where(allowed, scores, -jnp.inf)
        maximum = jnp.max(scores, axis=-1, keepdims=True)
        raised = jnp.exp(scores - maximum)
        denominator = jnp.sum(raised, axis=-1, keepdims=True)
        weights = (raised / denominator).astype(jnp.bfloat16)
        attended = jnp.einsum('rhqk,krhe->qrhe', weights.astype(jnp.float32), value_window.astype(jnp.float32))
        log_den = (maximum + jnp.log(denominator))[..., 0]
        return attended, jnp.transpose(log_den, (2, 0, 1))

    outputs, log_dens = lax.map(one_block, (jnp.arange(blocks, dtype=jnp.int32), grouped))
    return outputs.reshape(sequence_length, heads, HEAD_DIM), log_dens.reshape(sequence_length, heads)


def reference(queries, keys, values, w_out):
    sequence_length, columns = queries.shape
    group_results = [band_scores(queries, keys, values, dilation_step) for dilation_step in (1, MIDDLE_DILATION, FAR_DILATION)]
    stacked_out = jnp.stack([item[0] for item in group_results])
    stacked_den = jnp.stack([item[1] for item in group_results])
    shares = jax.nn.softmax(stacked_den, axis=0)
    attended = jnp.sum(shares[..., None] * stacked_out, axis=0).astype(jnp.bfloat16).reshape(sequence_length, columns)
    return jnp.dot(attended, w_out, preferred_element_type=jnp.float32).astype(jnp.bfloat16)
```

```python
import functools

import jax
import jax.numpy as jnp
from jax import lax
from jax.experimental import pallas as pl
from jax.experimental.pallas import tpu as pltpu
from jax.sharding import PartitionSpec as P

HEAD_DIM = 128
SIDE_KEY_COUNT = 64
MIDDLE_DILATION = 4
FAR_DILATION = 16
NEG = -1e30
LOG2E = 1.4426950408889634
EXP_SCALE = HEAD_DIM ** (-0.5) * LOG2E


def iota(shape, dim):
    return lax.broadcasted_iota(jnp.int32, shape, dim)


def class_major(rows):
    per = rows // FAR_DILATION
    out_row, in_row = iota((rows, rows), 0), iota((rows, rows), 1)
    return jnp.where(in_row == FAR_DILATION * (out_row % per) + out_row // per, 1.0, 0.0)


def token_order(rows):
    per = rows // FAR_DILATION
    out_row, in_row = iota((rows, rows), 0), iota((rows, rows), 1)
    return jnp.where(out_row == FAR_DILATION * (in_row % per) + in_row // per, 1.0, 0.0)


def dot(a, b):
    return jnp.dot(a, b, preferred_element_type=jnp.float32)


def dot_t(a, b):
    return lax.dot_general(a, b, (((1,), (1,)), ((), ())), preferred_element_type=jnp.float32)


def spread_kernel(group, arrays, *refs):
    ins, outs = refs[:arrays], refs[arrays:]
    me = lax.rem(lax.axis_index("sp"), group)
    order = class_major(ins[0].shape[0]).astype(jnp.bfloat16)
    for k in range(group):
        head = me ^ k
        cols = pl.ds(pl.multiple_of(head * HEAD_DIM, HEAD_DIM), HEAD_DIM)
        part = jnp.concatenate([ref[:, cols] for ref in ins], axis=1)
        outs[k][...] = dot(order, part).astype(jnp.bfloat16)


def spread(group, *arrays):
    rows = arrays[0].shape[0]
    out = jax.ShapeDtypeStruct((rows, HEAD_DIM * len(arrays)), jnp.bfloat16)
    return pl.pallas_call(
        functools.partial(spread_kernel, group, len(arrays)),
        out_shape=[out] * group,
        in_specs=[pl.BlockSpec(memory_space=pltpu.VMEM)] * len(arrays),
        out_specs=[pl.BlockSpec(memory_space=pltpu.VMEM)] * group,
        cost_estimate=pl.CostEstimate(flops=10**6, bytes_accessed=10**6, transcendentals=0),
    )(*arrays)


def attend_kernel(group, groups, *refs):
    q_in, kv_in = refs[:group], refs[group : 4 * group]
    outs = refs[4 * group : 5 * group]
    q_s, kv_s, num_s, top_s, den_s, out_s, bias16, bias4, bias1, sems = refs[5 * group :]
    rows = q_s.shape[1]
    per = rows // FAR_DILATION
    quarter = FAR_DILATION // MIDDLE_DILATION
    mid_rows = per * quarter
    here = lax.axis_index("sp")
    me, mine = lax.rem(here, group), here // group
    even = lax.rem(mine, 2) == 0
    first, last = mine == 0, mine == groups - 1

    copies = []
    for k in range(group):
        member = me ^ k
        copies.append(pltpu.make_async_copy(q_in[k], q_s.at[member], sems.at[k]))
        bases = (group, jnp.where(even, 2 * group, 0), jnp.where(even, 0, 2 * group))
        for j, base in enumerate(bases):
            slot = kv_s.at[base + member]
            copies.append(
                pltpu.make_async_copy(kv_in[j * group + k], slot, sems.at[(j + 1) * group + k])
            )
    for copy in copies:
        copy.start()

    side = SIDE_KEY_COUNT
    far_q, far_k = group * per, 3 * group * per
    q_pos, k_pos = iota((far_q, far_k), 0), iota((far_q, far_k), 1) - group * per
    near = jnp.abs(k_pos - q_pos) <= side
    near &= (k_pos >= jnp.where(first, 0, -far_q)) & (k_pos < jnp.where(last, far_q, 2 * far_q))
    bias16[...] = jnp.where(near, 0.0, NEG)

    q_row, k_row = iota((mid_rows, 3 * mid_rows), 0), iota((mid_rows, 3 * mid_rows), 1)
    q_pos = quarter * (q_row % per) + q_row // per
    k_pos = quarter * (k_row % per) + (k_row // per) % quarter + (k_row // mid_rows - 1) * mid_rows
    near = jnp.abs(k_pos - q_pos) <= side
    for b in range(group):
        ok = near
        if b == 0:
            ok &= k_pos >= jnp.where(first, 0, -mid_rows)
        if b == group - 1:
            ok &= k_pos < jnp.where(last, mid_rows, 2 * mid_rows)
        bias4[b] = jnp.where(ok, 0.0, NEG)

    q_row, k_row = iota((rows, rows), 0), iota((rows, rows), 1)
    q_pos = FAR_DILATION * (q_row % per) + q_row // per
    k_pos = FAR_DILATION * (k_row % per) + k_row // per
    bias1[:, :rows] = jnp.where(jnp.abs(k_pos - q_pos) <= side, 0.0, NEG)
    q_row, k_row = iota((rows, 2 * side), 0), iota((rows, 2 * side), 1)
    q_pos = FAR_DILATION * (q_row % per) + q_row // per
    k_pos = jnp.where(k_row < side, k_row - side, rows + k_row - side)
    bias1[:, rows:] = jnp.where(jnp.abs(k_pos - q_pos) <= side, 0.0, NEG)

    def scores_of(q, keys, bias):
        return dot_t(q, keys) + bias

    def weigh(scores, values, top):
        raised = jnp.exp2((scores - top) * EXP_SCALE).astype(jnp.bfloat16)
        both = dot(raised, jnp.concatenate([values, jnp.ones_like(values)], axis=1))
        return both[:, :HEAD_DIM], both[:, HEAD_DIM:]

    for copy in copies:
        copy.wait()

    def far(c, _):
        at = pl.ds(pl.multiple_of(c * per, per), per)
        q = q_s[:, at, :].reshape(far_q, HEAD_DIM)
        keys = kv_s[:, at, :HEAD_DIM].reshape(far_k, HEAD_DIM)
        values = kv_s[:, at, HEAD_DIM:].reshape(far_k, HEAD_DIM)
        scores = scores_of(q, keys, bias16[...])
        top = jnp.max(scores, axis=1, keepdims=True)
        num, den = weigh(scores, values, top)
        num_s[:, at, :] = num.reshape(group, per, HEAD_DIM)
        den_s[:, at, :] = den.reshape(group, per, HEAD_DIM)
        top_s[:, at, :] = jnp.broadcast_to(top, num.shape).reshape(group, per, HEAD_DIM)
        return 0

    lax.fori_loop(0, FAR_DILATION, far, 0, unroll=4)

    def join(old, new):
        (num_a, den_a, top_a), (num_b, den_b, top_b) = old, new
        top = jnp.maximum(top_a, top_b)
        by_a, by_b = jnp.exp2((top_a - top) * EXP_SCALE), jnp.exp2((top_b - top) * EXP_SCALE)
        return num_a * by_a + num_b * by_b, den_a * by_a + den_b * by_b, top

    def middle(step, _):
        b = step // MIDDLE_DILATION
        residue = lax.rem(step, MIDDLE_DILATION)
        ats = [
            pl.ds(pl.multiple_of((MIDDLE_DILATION * s + residue) * per, per), per)
            for s in range(quarter)
        ]
        q = jnp.concatenate([q_s[b, at, :] for at in ats], axis=0)
        slots = [group - 1 + b + j for j in range(3)]
        keys = jnp.concatenate([kv_s[j, at, :HEAD_DIM] for j in slots for at in ats], axis=0)
        values = jnp.concatenate([kv_s[j, at, HEAD_DIM:] for j in slots for at in ats], axis=0)
        scores = scores_of(q, keys, bias4[b])
        top = jnp.max(scores, axis=1, keepdims=True)
        num, den = weigh(scores, values, top)
        old = [jnp.concatenate([ref[b, at, :] for at in ats], axis=0) for ref in (num_s, den_s, top_s)]
        new = join(old, (num, den, top))
        for ref, value in zip((num_s, den_s, top_s), new):
            for s, at in enumerate(ats):
                ref[b, at, :] = value[s * per : (s + 1) * per]
        return 0

    lax.fori_loop(0, group * MIDDLE_DILATION, middle, 0, unroll=4)

    token = iota((side, rows), 0)
    column = iota((side, rows), 1)
    column = FAR_DILATION * (column % per) + column // per
    ends = jnp.where(column == token, 1.0, 0.0).astype(jnp.bfloat16)
    tails = jnp.where(column == token + rows - side, 1.0, 0.0).astype(jnp.bfloat16)
    natural = token_order(rows).astype(jnp.bfloat16)
    half = rows // 2
    for b in range(group):
        own = kv_s[group + b]
        beside = jnp.concatenate([dot(tails, kv_s[group + b - 1]), dot(ends, kv_s[group + b + 1])], axis=0)
        beside = beside.astype(jnp.bfloat16)
        values = jnp.concatenate([own[:, HEAD_DIM:], beside[:, HEAD_DIM:]], axis=0)
        column = iota((1, 2 * side), 1)
        edge = jnp.zeros((1, 2 * side), jnp.float32)
        if b == 0:
            edge += jnp.where((column < side) & first, NEG, 0.0)
        if b == group - 1:
            edge += jnp.where((column >= side) & last, NEG, 0.0)
        for part in range(2):
            at = pl.ds(part * half, half)
            q = q_s[b, at, :]
            inner = scores_of(q, own[:, :HEAD_DIM], bias1[at, :rows])
            outer = scores_of(q, beside[:, :HEAD_DIM], bias1[at, rows:])
            if b in (0, group - 1):
                outer += edge
            scores = jnp.concatenate([inner, outer], axis=1)
            top = jnp.max(scores, axis=1, keepdims=True)
            num, den = weigh(scores, values, top)
            num, den, _ = join((num_s[b, at, :], den_s[b, at, :], top_s[b, at, :]), (num, den, top))
            out_s[b, at, :] = (num / den).astype(jnp.bfloat16)
    for k in range(group):
        outs[k][...] = dot(natural, out_s[me ^ k]).astype(jnp.bfloat16)


def attend(group, groups, q, own, even, odd):
    rows = q[0].shape[0]
    per = rows // FAR_DILATION
    mid_rows = per * (FAR_DILATION // MIDDLE_DILATION)
    f32, bf16 = jnp.float32, jnp.bfloat16
    return pl.pallas_call(
        functools.partial(attend_kernel, group, groups),
        out_shape=[jax.ShapeDtypeStruct((rows, HEAD_DIM), bf16)] * group,
        in_specs=[pl.BlockSpec(memory_space=pl.ANY)] * (4 * group),
        out_specs=[pl.BlockSpec(memory_space=pltpu.VMEM)] * group,
        scratch_shapes=[
            pltpu.VMEM((group, rows, HEAD_DIM), bf16),
            pltpu.VMEM((3 * group, rows, 2 * HEAD_DIM), bf16),
            pltpu.VMEM((group, rows, HEAD_DIM), f32),
            pltpu.VMEM((group, rows, HEAD_DIM), f32),
            pltpu.VMEM((group, rows, HEAD_DIM), f32),
            pltpu.VMEM((group, rows, HEAD_DIM), bf16),
            pltpu.VMEM((group * per, 3 * group * per), f32),
            pltpu.VMEM((group, mid_rows, 3 * mid_rows), f32),
            pltpu.VMEM((rows, rows + 2 * SIDE_KEY_COUNT), f32),
            pltpu.SemaphoreType.DMA((4 * group,)),
        ],
        cost_estimate=pl.CostEstimate(flops=10**9, bytes_accessed=10**6, transcendentals=10**6),
    )(*q, *own, *even, *odd)


def project_kernel(group, *refs):
    own, other = refs[:group], refs[group : 2 * group]
    w_ref, out_ref = refs[2 * group :]
    me, side = lax.rem(lax.axis_index("sp"), group), lax.axis_index("tp")
    total = None
    for k in range(group):
        left = jnp.concatenate([own[k][...], other[k][...]], axis=1)
        right = []
        for core in (side, 1 - side):
            row = (core * group + (me ^ k)) * HEAD_DIM
            right.append(w_ref[pl.ds(pl.multiple_of(row, HEAD_DIM), HEAD_DIM), :])
        term = dot(left, jnp.concatenate(right, axis=0))
        total = term if total is None else total + term
    out_ref[...] = total.astype(jnp.bfloat16)


def project(group, own, other, w_out):
    rows, width = own[0].shape[0], w_out.shape[1]
    tile = 256
    piece = pl.BlockSpec((rows, HEAD_DIM), lambda j: (0, 0))
    return pl.pallas_call(
        functools.partial(project_kernel, group),
        out_shape=jax.ShapeDtypeStruct((rows, width), jnp.bfloat16),
        grid=(width // tile,),
        in_specs=[piece] * (2 * group) + [pl.BlockSpec((w_out.shape[0], tile), lambda j: (0, j))],
        out_specs=pl.BlockSpec((rows, tile), lambda j: (0, j)),
        cost_estimate=pl.CostEstimate(flops=10**9, bytes_accessed=10**6, transcendentals=0),
    )(*own, *other, w_out)


def per_device(queries, keys, values, w_out):
    rows = queries.shape[0]
    shards = lax.axis_size("sp")
    group = -(-(SIDE_KEY_COUNT * FAR_DILATION) // rows)
    groups = shards // group

    def inside(value, k):
        return lax.ppermute(value, "sp", [(s, s ^ k) for s in range(shards)])

    def across(value, parity):
        pairs = []
        for s in range(shards):
            mine = s // group
            beside = mine + 1 if mine % 2 == parity else mine - 1
            for t in range(2):
                if 0 <= beside < groups:
                    pairs.append((2 * s + t, 2 * (s + (beside - mine) * group) + t))
                else:
                    pairs.append((2 * s + t, 2 * s + 1 - t))
        return lax.ppermute(value, ("sp", "tp"), pairs)

    def other_core(value):
        return lax.ppermute(value, "tp", [(0, 1), (1, 0)])

    kv = spread(group, keys, values)
    q = spread(group, queries)
    own = [kv[0]] + [inside(kv[k], k) for k in range(1, group)]
    even = [across(piece, 0) for piece in own]
    odd = [across(piece, 1) for piece in own]
    q = [q[0]] + [inside(q[k], k) for k in range(1, group)]
    out = attend(group, groups, q, own, even, odd)
    out = [out[0]] + [inside(out[k], k) for k in range(1, group)]
    return project(group, out, [other_core(piece) for piece in out], w_out)


def solution(mesh):
    in_specs = (P("sp", "tp"), P("sp", "tp"), P("sp", "tp"), P(None, "tp"))
    out_specs = P("sp", "tp")
    return jax.shard_map(
        per_device, mesh=mesh, in_specs=in_specs, out_specs=out_specs, check_vma=False
    )
```

```python
import functools

import jax
import jax.numpy as jnp
from jax import lax
from jax.experimental import pallas as pl
from jax.experimental.pallas import tpu as pltpu
from jax.sharding import PartitionSpec as P

HEAD_DIM = 128
SIDE_KEY_COUNT = 64
MIDDLE_DILATION = 4
FAR_DILATION = 16
NEG = -1e30
VMEM_LIMIT = 16 * 2**20
LOCAL_FLOPS = 10**9
LOG2E = 1.4426950408889634
EXP_SCALE = HEAD_DIM ** (-0.5) * LOG2E


def iota(shape, dim):
    return lax.broadcasted_iota(jnp.int32, shape, dim)


def class_major(rows):
    per = rows // FAR_DILATION
    out_row, in_row = iota((rows, rows), 0), iota((rows, rows), 1)
    return jnp.where(in_row == FAR_DILATION * (out_row % per) + out_row // per, 1.0, 0.0)


def token_order(rows):
    per = rows // FAR_DILATION
    out_row, in_row = iota((rows, rows), 0), iota((rows, rows), 1)
    return jnp.where(out_row == FAR_DILATION * (in_row % per) + in_row // per, 1.0, 0.0)


def dot(a, b):
    return jnp.dot(a, b, preferred_element_type=jnp.float32)


def dot_t(a, b):
    return lax.dot_general(a, b, (((1,), (1,)), ((), ())), preferred_element_type=jnp.float32)


def spread_kernel(group, arrays, *refs):
    ins, outs = refs[:arrays], refs[arrays:]
    me = lax.rem(lax.axis_index("sp"), group)
    order = class_major(ins[0].shape[0]).astype(jnp.bfloat16)
    for k in range(group):
        head = me ^ k
        cols = pl.ds(pl.multiple_of(head * HEAD_DIM, HEAD_DIM), HEAD_DIM)
        part = jnp.concatenate([ref[:, cols] for ref in ins], axis=1)
        outs[k][...] = dot(order, part).astype(jnp.bfloat16)


def spread(group, *arrays):
    rows = arrays[0].shape[0]
    out = jax.ShapeDtypeStruct((rows, HEAD_DIM * len(arrays)), jnp.bfloat16)
    return pl.pallas_call(
        functools.partial(spread_kernel, group, len(arrays)),
        out_shape=[out] * group,
        in_specs=[pl.BlockSpec(memory_space=pltpu.VMEM)] * len(arrays),
        out_specs=[pl.BlockSpec(memory_space=pltpu.VMEM)] * group,
        compiler_params=pltpu.CompilerParams(vmem_limit_bytes=VMEM_LIMIT),
        cost_estimate=pl.CostEstimate(flops=10**6, bytes_accessed=10**6, transcendentals=0),
    )(*arrays)


def far_bias(queries, keys, offset, valid):
    q_pos, k_pos = iota((queries, keys), 0), iota((queries, keys), 1) + offset
    near = jnp.abs(k_pos - q_pos) <= SIDE_KEY_COUNT
    return jnp.where(near & valid, 0.0, NEG)


def middle_place(row, per):
    quarter = FAR_DILATION // MIDDLE_DILATION
    return quarter * (row % per) + (row // per) % quarter


def token_place(row, per):
    return FAR_DILATION * (row % per) + row // per


def band(q_pos, k_pos):
    return jnp.where(jnp.abs(k_pos - q_pos) <= SIDE_KEY_COUNT, 0.0, NEG)


def pick_tokens(rows, start, count):
    column = token_place(iota((count, rows), 1), rows // FAR_DILATION)
    return jnp.where(column == iota((count, rows), 0) + start, 1.0, 0.0).astype(jnp.bfloat16)


def residue_rows(residue, per):
    quarter = FAR_DILATION // MIDDLE_DILATION
    return [pl.ds((MIDDLE_DILATION * s + residue) * per, per) for s in range(quarter)]


def softmax_parts(units):
    scores = [dot_t(q, k) + bias for q, k, _, bias in units]
    tops = [jnp.max(s, axis=1, keepdims=True) for s in scores]
    raised = [jnp.exp2((s - t) * EXP_SCALE).astype(jnp.bfloat16) for s, t in zip(scores, tops)]
    both = [
        dot(r, jnp.concatenate([v, jnp.ones_like(v)], axis=1))
        for r, (_, _, v, _) in zip(raised, units)
    ]
    return [
        (x[:, :HEAD_DIM], x[:, HEAD_DIM:], jnp.broadcast_to(t, (x.shape[0], HEAD_DIM)))
        for x, t in zip(both, tops)
    ]


def join(old, new):
    (num_a, den_a, top_a), (num_b, den_b, top_b) = old, new
    top = jnp.maximum(top_a, top_b)
    by_a, by_b = jnp.exp2((top_a - top) * EXP_SCALE), jnp.exp2((top_b - top) * EXP_SCALE)
    return num_a * by_a + num_b * by_b, den_a * by_a + den_b * by_b, top


def local_kernel(group, *refs):
    q_in, kv_in = refs[:group], refs[group : 2 * group]
    q_s, num_s, den_s, top_s = refs[2 * group : 2 * group + 4]
    kv_s, bias1, sems = refs[2 * group + 4 :]
    rows = q_s.shape[1]
    per = rows // FAR_DILATION
    quarter = FAR_DILATION // MIDDLE_DILATION
    part = per * quarter
    side = SIDE_KEY_COUNT
    me = lax.rem(lax.axis_index("sp"), group)
    stats = (num_s, den_s, top_s)

    copies = []
    for k in range(group):
        copies.append(pltpu.make_async_copy(q_in[k], q_s.at[me ^ k], sems.at[k]))
        copies.append(pltpu.make_async_copy(kv_in[k], kv_s.at[me ^ k], sems.at[group + k]))
    for copy in copies:
        copy.start()

    far = far_bias(group * per, group * per, 0, True)
    q_pos = middle_place(iota((part, 3 * part), 0), per)
    column = iota((part, 3 * part), 1)
    middle = band(q_pos, middle_place(column, per) + (column // part - 1) * part)
    q_pos = token_place(iota((rows, rows), 0), per)
    bias1[:, :rows] = band(q_pos, token_place(iota((rows, rows), 1), per))
    q_pos, column = token_place(iota((rows, 2 * side), 0), per), iota((rows, 2 * side), 1)
    bias1[:, rows:] = band(q_pos, jnp.where(column < side, column - side, rows + column - side))
    tails, heads = pick_tokens(rows, rows - side, side), pick_tokens(rows, 0, side)

    for copy in copies:
        copy.wait()

    batch = 8
    for first in range(0, FAR_DILATION, batch):
        ats = [pl.ds(c * per, per) for c in range(first, first + batch)]
        units = []
        for at in ats:
            q = q_s[:, at, :].reshape(group * per, HEAD_DIM)
            kv = kv_s[:, at, :].reshape(group * per, 2 * HEAD_DIM)
            units.append((q, kv[:, :HEAD_DIM], kv[:, HEAD_DIM:], far))
        for at, found in zip(ats, softmax_parts(units)):
            for ref, value in zip(stats, found):
                ref[:, at, :] = value.reshape(group, per, HEAD_DIM)

    for b in range(group):
        low, high = max(b - 1, 0), min(b + 2, group)
        columns = slice((low - b + 1) * part, (high - b + 1) * part)
        units, places = [], []
        for residue in range(MIDDLE_DILATION):
            ats = residue_rows(residue, per)
            q = jnp.concatenate([q_s[b, at, :] for at in ats], axis=0)
            kv = jnp.concatenate([kv_s[j, at, :] for j in range(low, high) for at in ats], axis=0)
            units.append((q, kv[:, :HEAD_DIM], kv[:, HEAD_DIM:], middle[:, columns]))
            places.append(ats)
        for ats, found in zip(places, softmax_parts(units)):
            old = [jnp.concatenate([ref[b, at, :] for at in ats], axis=0) for ref in stats]
            for ref, value in zip(stats, join(old, found)):
                for s, at in enumerate(ats):
                    ref[b, at, :] = value[s * per : (s + 1) * per]

    half = rows // 2
    for b in range(group):
        pieces, biases = [kv_s[b]], [bias1[:, :rows]]
        if b > 0:
            pieces.append(dot(tails, kv_s[b - 1]).astype(jnp.bfloat16))
        if b < group - 1:
            pieces.append(dot(heads, kv_s[b + 1]).astype(jnp.bfloat16))
        kv = jnp.concatenate(pieces, axis=0)
        low = rows if b > 0 else rows + side
        bias = jnp.concatenate([bias1[:, :rows], bias1[:, low : low + kv.shape[0] - rows]], axis=1)
        units = [
            (q_s[b, pl.ds(p * half, half), :], kv[:, :HEAD_DIM], kv[:, HEAD_DIM:], bias[p * half : (p + 1) * half])
            for p in range(2)
        ]
        for p, found in enumerate(softmax_parts(units)):
            at = pl.ds(p * half, half)
            for ref, value in zip(stats, join([ref[b, at, :] for ref in stats], found)):
                ref[b, at, :] = value


def halo_kernel(group, groups, *refs):
    q_in, num_in, den_in, top_in = refs[:4]
    kv_in, outs = refs[4 : 4 + 2 * group], refs[4 + 2 * group : 4 + 3 * group]
    q_s, num_s, den_s, top_s, kv_s, out_s, sems = refs[4 + 3 * group :]
    rows = q_s.shape[1]
    per = rows // FAR_DILATION
    quarter = FAR_DILATION // MIDDLE_DILATION
    part = per * quarter
    side = SIDE_KEY_COUNT
    here = lax.axis_index("sp")
    me, mine = lax.rem(here, group), here // group
    even = lax.rem(mine, 2) == 0
    has_before, has_after = mine > 0, mine < groups - 1
    stats = (num_s, den_s, top_s)

    copies = []
    for j, (source, target) in enumerate(zip((q_in, num_in, den_in, top_in), (q_s,) + stats)):
        copies.append(pltpu.make_async_copy(source, target, sems.at[j]))
    for j, base in enumerate((jnp.where(even, group, 0), jnp.where(even, 0, group))):
        for k in range(group):
            slot = kv_s.at[base + (me ^ k)]
            copies.append(pltpu.make_async_copy(kv_in[j * group + k], slot, sems.at[4 + j * group + k]))
    for copy in copies:
        copy.start()

    steps = group * per
    far = jnp.concatenate(
        [far_bias(steps, steps, -steps, has_before), far_bias(steps, steps, steps, has_after)], axis=1
    )
    column = iota((part, part), 1)
    q_mid, k_mid = middle_place(iota((part, part), 0), per), middle_place(column, per)
    before = jnp.where(has_before, band(q_mid, k_mid - part), NEG)
    after = jnp.where(has_after, band(q_mid, k_mid + part), NEG)
    near = []
    for residue in range(MIDDLE_DILATION):
        row, token = iota((part, side), 0), iota((part, side), 1)
        q_pos = FAR_DILATION * (row % per) + MIDDLE_DILATION * (row // per) + residue
        near.append(
            (
                jnp.where(has_before, band(q_pos, token - side), NEG),
                jnp.where(has_after, band(q_pos, token + rows), NEG),
            )
        )
    tails, heads = pick_tokens(rows, rows - side, side), pick_tokens(rows, 0, side)
    natural = token_order(rows).astype(jnp.bfloat16)

    for copy in copies:
        copy.wait()

    tail = dot(tails, kv_s[group - 1]).astype(jnp.bfloat16)
    head = dot(heads, kv_s[group]).astype(jnp.bfloat16)
    units, places = [], []
    for b, slot, ends, mid, which in ((0, group - 1, tail, before, 0), (group - 1, group, head, after, 1)):
        for residue in range(MIDDLE_DILATION):
            ats = residue_rows(residue, per)
            q = jnp.concatenate([q_s[b, at, :] for at in ats], axis=0)
            kv = jnp.concatenate([kv_s[slot, at, :] for at in ats] + [ends], axis=0)
            bias = jnp.concatenate([mid, near[residue][which]], axis=1)
            units.append((q, kv[:, :HEAD_DIM], kv[:, HEAD_DIM:], bias))
            places.append((b, ats))
    for (b, ats), found in zip(places, softmax_parts(units)):
        old = [jnp.concatenate([ref[b, at, :] for at in ats], axis=0) for ref in stats]
        for ref, value in zip(stats, join(old, found)):
            for s, at in enumerate(ats):
                ref[b, at, :] = value[s * per : (s + 1) * per]

    batch = 8
    for first in range(0, FAR_DILATION, batch):
        ats = [pl.ds(c * per, per) for c in range(first, first + batch)]
        units = []
        for at in ats:
            q = q_s[:, at, :].reshape(steps, HEAD_DIM)
            kv = kv_s[:, at, :].reshape(2 * steps, 2 * HEAD_DIM)
            units.append((q, kv[:, :HEAD_DIM], kv[:, HEAD_DIM:], far))
        for at, found in zip(ats, softmax_parts(units)):
            old = [ref[:, at, :].reshape(steps, HEAD_DIM) for ref in stats]
            num, den, _ = join(old, found)
            out_s[:, at, :] = (num / den).astype(jnp.bfloat16).reshape(group, per, HEAD_DIM)
    for k in range(group):
        outs[k][...] = dot(natural, out_s[me ^ k]).astype(jnp.bfloat16)


def attend_local(group, q, own):
    rows = q[0].shape[0]
    f32, bf16 = jnp.float32, jnp.bfloat16
    shape = (group, rows, HEAD_DIM)
    return pl.pallas_call(
        functools.partial(local_kernel, group),
        out_shape=[jax.ShapeDtypeStruct(shape, kind) for kind in (bf16, f32, f32, f32)],
        in_specs=[pl.BlockSpec(memory_space=pl.ANY)] * (2 * group),
        out_specs=[pl.BlockSpec(memory_space=pltpu.VMEM)] * 4,
        scratch_shapes=[
            pltpu.VMEM((group, rows, 2 * HEAD_DIM), bf16),
            pltpu.VMEM((rows, rows + 2 * SIDE_KEY_COUNT), f32),
            pltpu.SemaphoreType.DMA((2 * group,)),
        ],
        compiler_params=pltpu.CompilerParams(vmem_limit_bytes=VMEM_LIMIT),
        cost_estimate=pl.CostEstimate(flops=LOCAL_FLOPS, bytes_accessed=10**6, transcendentals=0),
    )(*q, *own)


def attend_halo(group, groups, found, even, odd):
    q = found[0]
    rows = q.shape[1]
    f32, bf16 = jnp.float32, jnp.bfloat16
    shape = (group, rows, HEAD_DIM)
    return pl.pallas_call(
        functools.partial(halo_kernel, group, groups),
        out_shape=[jax.ShapeDtypeStruct((rows, HEAD_DIM), bf16)] * group,
        in_specs=[pl.BlockSpec(memory_space=pl.ANY)] * (4 + 2 * group),
        out_specs=[pl.BlockSpec(memory_space=pltpu.VMEM)] * group,
        scratch_shapes=[
            pltpu.VMEM(shape, bf16),
            pltpu.VMEM(shape, f32),
            pltpu.VMEM(shape, f32),
            pltpu.VMEM(shape, f32),
            pltpu.VMEM((2 * group, rows, 2 * HEAD_DIM), bf16),
            pltpu.VMEM(shape, bf16),
            pltpu.SemaphoreType.DMA((4 + 2 * group,)),
        ],
        compiler_params=pltpu.CompilerParams(vmem_limit_bytes=VMEM_LIMIT),
        cost_estimate=pl.CostEstimate(flops=10**9, bytes_accessed=10**6, transcendentals=0),
    )(*found, *even, *odd)


def project_kernel(group, *refs):
    own, other = refs[:group], refs[group : 2 * group]
    w_ref, out_ref = refs[2 * group :]
    me, side = lax.rem(lax.axis_index("sp"), group), lax.axis_index("tp")
    total = None
    for k in range(group):
        left = jnp.concatenate([own[k][...], other[k][...]], axis=1)
        right = []
        for core in (side, 1 - side):
            row = (core * group + (me ^ k)) * HEAD_DIM
            right.append(w_ref[pl.ds(pl.multiple_of(row, HEAD_DIM), HEAD_DIM), :])
        term = dot(left, jnp.concatenate(right, axis=0))
        total = term if total is None else total + term
    out_ref[...] = total.astype(jnp.bfloat16)


def project(group, own, other, w_out):
    rows, width = own[0].shape[0], w_out.shape[1]
    return pl.pallas_call(
        functools.partial(project_kernel, group),
        out_shape=jax.ShapeDtypeStruct((rows, width), jnp.bfloat16),
        in_specs=[pl.BlockSpec(memory_space=pltpu.VMEM)] * (2 * group + 1),
        out_specs=pl.BlockSpec(memory_space=pltpu.VMEM),
        compiler_params=pltpu.CompilerParams(vmem_limit_bytes=VMEM_LIMIT),
        cost_estimate=pl.CostEstimate(flops=10**9, bytes_accessed=10**6, transcendentals=0),
    )(*own, *other, w_out)


def per_device(queries, keys, values, w_out):
    rows = queries.shape[0]
    shards = lax.axis_size("sp")
    group = -(-(SIDE_KEY_COUNT * FAR_DILATION) // rows)
    groups = shards // group

    def inside(value, k):
        return lax.ppermute(value, "sp", [(s, s ^ k) for s in range(shards)])

    def across(value, parity):
        pairs = []
        for s in range(shards):
            mine = s // group
            beside = mine + 1 if mine % 2 == parity else mine - 1
            for t in range(2):
                if 0 <= beside < groups:
                    pairs.append((2 * s + t, 2 * (s + (beside - mine) * group) + t))
                else:
                    pairs.append((2 * s + t, 2 * s + 1 - t))
        return lax.ppermute(value, ("sp", "tp"), pairs)

    def other_core(value):
        return lax.ppermute(value, "tp", [(0, 1), (1, 0)])

    kv = spread(group, keys, values)
    q = spread(group, queries)
    own = [kv[0]] + [inside(kv[k], k) for k in range(1, group)]
    even = [across(piece, 0) for piece in own]
    odd = [across(piece, 1) for piece in own]
    q = [q[0]] + [inside(q[k], k) for k in range(1, group)]
    out = attend_halo(group, groups, attend_local(group, q, own), even, odd)
    out = [out[0]] + [inside(out[k], k) for k in range(1, group)]
    return project(group, out, [other_core(piece) for piece in out], w_out)


def solution(mesh):
    in_specs = (P("sp", "tp"), P("sp", "tp"), P("sp", "tp"), P(None, "tp"))
    out_specs = P("sp", "tp")
    return jax.shard_map(
        per_device, mesh=mesh, in_specs=in_specs, out_specs=out_specs, check_vma=False
    )
```

```python
import functools

import jax
import jax.numpy as jnp
from jax import lax
from jax.experimental import pallas as pl
from jax.experimental.pallas import tpu as pltpu
from jax.sharding import PartitionSpec as P


HEAD_DIM = 128
SIDE_KEY_COUNT = 64
MIDDLE_DILATION = 4
FAR_DILATION = 16
NEG = -1e30
VMEM_LIMIT = 16 * 2**20
SPREAD_VMEM_LIMIT = 53 * 2**20
LOCAL_FLOPS = 2 * 10**9
LOG2E = 1.4426950408889634
EXP_SCALE = HEAD_DIM ** (-0.5) * LOG2E


def iota(shape, dim):
    return lax.broadcasted_iota(jnp.int32, shape, dim)


def class_major(rows):
    per = rows // FAR_DILATION
    out_row, in_row = iota((rows, rows), 0), iota((rows, rows), 1)
    return jnp.where(in_row == FAR_DILATION * (out_row % per) + out_row // per, 1.0, 0.0)


def token_order(rows):
    per = rows // FAR_DILATION
    out_row, in_row = iota((rows, rows), 0), iota((rows, rows), 1)
    return jnp.where(out_row == FAR_DILATION * (in_row % per) + in_row // per, 1.0, 0.0)


def dot(a, b):
    return jnp.dot(a, b, preferred_element_type=jnp.float32)


def dot_t(a, b):
    return lax.dot_general(a, b, (((1,), (1,)), ((), ())), preferred_element_type=jnp.float32)


def spread_kernel(group, *refs):
    ins, outs = refs[:3], refs[3:-4]
    keys, values, queries, sems = refs[-4:]
    kv_out, q_out = outs[:group], outs[group:]
    copies = [
        pltpu.make_async_copy(source, target, sems.at[j])
        for j, (source, target) in enumerate(zip(ins, (keys, values, queries)))
    ]
    for copy in copies:
        copy.start()
    me = lax.rem(lax.axis_index("sp"), group)
    order = class_major(keys.shape[0]).astype(jnp.bfloat16)

    def columns(ref, k):
        return ref[:, pl.ds(pl.multiple_of((me ^ k) * HEAD_DIM, HEAD_DIM), HEAD_DIM)]

    for copy in copies:
        copy.wait()
    for k in range(group):
        part = jnp.concatenate([columns(keys, k), columns(values, k)], axis=1)
        kv_out[k][:, : 2 * HEAD_DIM] = dot(order, part).astype(jnp.bfloat16)
    q_out = iter(q_out)
    for k in range(group):
        part = dot(order, columns(queries, k)).astype(jnp.bfloat16)
        if k in MERGED:
            kv_out[k][:, 2 * HEAD_DIM :] = part
        else:
            next(q_out)[...] = part


def spread(group, keys, values, queries):
    rows = keys.shape[0]

    def shape(width):
        return jax.ShapeDtypeStruct((rows, width * HEAD_DIM), jnp.bfloat16)

    shapes = [shape(3 if k in MERGED else 2) for k in range(group)]
    shapes += [shape(1)] * (group - len(MERGED))
    found = pl.pallas_call(
        functools.partial(spread_kernel, group),
        out_shape=shapes,
        in_specs=[pl.BlockSpec(memory_space=pltpu.HBM)] * 3,
        out_specs=[pl.BlockSpec(memory_space=pltpu.VMEM)] * len(shapes),
        scratch_shapes=[pltpu.VMEM(keys.shape, jnp.bfloat16)] * 3 + [pltpu.SemaphoreType.DMA((3,))],
        compiler_params=pltpu.CompilerParams(vmem_limit_bytes=SPREAD_VMEM_LIMIT),
        cost_estimate=pl.CostEstimate(flops=10**6, bytes_accessed=10**6, transcendentals=0),
    )(keys, values, queries)
    return found[:group], dict(zip([k for k in range(group) if k not in MERGED], found[group:]))


def pile_kernel(*refs):
    rows, width = refs[0].shape[0], refs[-1].shape[1]
    for j, ref in enumerate(refs[:-1]):
        refs[-1][j * rows : (j + 1) * rows] = ref[:, :width]


def pile(pieces):
    if len(pieces) == 1 and pieces[0].shape[1] == 2 * HEAD_DIM:
        return pieces[0]
    rows = pieces[0].shape[0] * len(pieces)
    return pl.pallas_call(
        pile_kernel,
        out_shape=jax.ShapeDtypeStruct((rows, 2 * HEAD_DIM), pieces[0].dtype),
        in_specs=[pl.BlockSpec(memory_space=pltpu.VMEM)] * len(pieces),
        out_specs=pl.BlockSpec(memory_space=pltpu.VMEM),
        compiler_params=pltpu.CompilerParams(vmem_limit_bytes=VMEM_LIMIT),
        cost_estimate=pl.CostEstimate(flops=10**6, bytes_accessed=10**6, transcendentals=0),
    )(*pieces)


def middle_place(row, per):
    quarter = FAR_DILATION // MIDDLE_DILATION
    return quarter * (row % per) + (row // per) % quarter


def token_place(row, per):
    return FAR_DILATION * (row % per) + row // per


def band(q_pos, k_pos):
    return jnp.where(jnp.abs(k_pos - q_pos) <= SIDE_KEY_COUNT, 0.0, NEG)


def pick_tokens(rows, start, count):
    column = token_place(iota((count, rows), 1), rows // FAR_DILATION)
    return jnp.where(column == iota((count, rows), 0) + start, 1.0, 0.0).astype(jnp.bfloat16)


def residue_rows(residue, per):
    quarter = FAR_DILATION // MIDDLE_DILATION
    return [pl.ds((MIDDLE_DILATION * s + residue) * per, per) for s in range(quarter)]


def softmax_parts(units):
    scores = [dot_t(q, k) + bias for q, k, _, bias in units]
    tops = [jnp.max(s, axis=1, keepdims=True) for s in scores]
    raised = [jnp.exp2((s - t) * EXP_SCALE).astype(jnp.bfloat16) for s, t in zip(scores, tops)]
    both = [
        dot(r, jnp.concatenate([v, jnp.ones_like(v)], axis=1))
        for r, (_, _, v, _) in zip(raised, units)
    ]
    return [
        (x[:, :HEAD_DIM], x[:, HEAD_DIM:], jnp.broadcast_to(t, (x.shape[0], HEAD_DIM)))
        for x, t in zip(both, tops)
    ]


def join(old, new):
    (num_a, den_a, top_a), (num_b, den_b, top_b) = old, new
    top = jnp.maximum(top_a, top_b)
    by_a, by_b = jnp.exp2((top_a - top) * EXP_SCALE), jnp.exp2((top_b - top) * EXP_SCALE)
    return num_a * by_a + num_b * by_b, den_a * by_a + den_b * by_b, top


def mask_kernel(group, groups, *refs):
    far_own, middle_own, near_own, far_halo, touch_halo, ends = refs
    rows = near_own.shape[0]
    per = rows // FAR_DILATION
    quarter = FAR_DILATION // MIDDLE_DILATION
    part = per * quarter
    side = SIDE_KEY_COUNT
    here = lax.axis_index("sp")
    me, mine = lax.rem(here, group), here // group
    even = lax.rem(mine, 2) == 0
    before = jnp.where(mine > 0, 0.0, NEG)
    after = jnp.where(mine < groups - 1, 0.0, NEG)

    steps = group * per
    far_own[...] = band(iota((steps, steps), 0), iota((steps, steps), 1))
    column = iota((part, 4 * part), 1)
    q_pos, k_pos = middle_place(iota((part, 4 * part), 0), per), middle_place(column, per)
    shard = jnp.where(column // part == 1, part, jnp.where(column // part == 2, -part, 0))
    middle_own[...] = band(q_pos, k_pos + shard)
    q_pos = token_place(iota((rows, rows), 0), per)
    near_own[:, :rows] = band(q_pos, token_place(iota((rows, rows), 1), per))
    q_pos, column = token_place(iota((rows, 2 * side), 0), per), iota((rows, 2 * side), 1)
    near_own[:, rows:] = band(q_pos, jnp.where(column < side, column - side, rows + column - side))

    column = iota((steps, 2 * steps), 1)
    place = ((column % steps) // per ^ me) * per + column % per
    behind = column // steps == jnp.where(even, 1, 0)
    k_pos = place + jnp.where(behind, -steps, steps)
    far_halo[...] = band(iota((steps, 2 * steps), 0), k_pos) + jnp.where(behind, before, after)
    q_mid, k_mid = middle_place(iota((part, part), 0), per), middle_place(iota((part, part), 1), per)
    row, token = iota((part, side), 0), iota((part, side), 1)
    for slot, (valid, step, start) in enumerate(((before, -part, -side), (after, part, rows))):
        for residue in range(MIDDLE_DILATION):
            q_pos = FAR_DILATION * (row % per) + MIDDLE_DILATION * (row // per) + residue
            touch_halo[slot, residue, :, :part] = band(q_mid, k_mid + step) + valid
            touch_halo[slot, residue, :, part:] = band(q_pos, token + start) + valid
    ends[0] = pick_tokens(rows, rows - side, side)
    ends[1] = pick_tokens(rows, 0, side)


def masks(group, groups, rows):
    per = rows // FAR_DILATION
    part = per * (FAR_DILATION // MIDDLE_DILATION)
    steps, side = group * per, SIDE_KEY_COUNT
    shapes = [
        (steps, steps),
        (part, 4 * part),
        (rows, rows + 2 * side),
        (steps, 2 * steps),
        (2, MIDDLE_DILATION, part, part + side),
    ]
    shapes = [jax.ShapeDtypeStruct(shape, jnp.float32) for shape in shapes]
    return pl.pallas_call(
        functools.partial(mask_kernel, group, groups),
        out_shape=shapes + [jax.ShapeDtypeStruct((2, side, rows), jnp.bfloat16)],
        out_specs=[pl.BlockSpec(memory_space=pltpu.VMEM)] * 6,
        compiler_params=pltpu.CompilerParams(vmem_limit_bytes=VMEM_LIMIT),
        cost_estimate=pl.CostEstimate(flops=10**6, bytes_accessed=10**6, transcendentals=0),
    )()


def local_kernel(group, *refs):
    kv_in, q_in, refs = refs[:group], refs[group:-9], refs[-9:]
    far_own, middle_own, bias1, ends, q_s, num_s, den_s, top_s, kv_s = refs
    rows = q_s.shape[1]
    per = rows // FAR_DILATION
    quarter = FAR_DILATION // MIDDLE_DILATION
    part = per * quarter
    side = SIDE_KEY_COUNT
    me = lax.rem(lax.axis_index("sp"), group)
    stats = (num_s, den_s, top_s)
    q_in = iter(q_in)
    for k in range(group):
        q_s[me ^ k] = kv_in[k][:, 2 * HEAD_DIM :] if k in MERGED else next(q_in)[...]
        kv_s[me ^ k] = kv_in[k][:, : 2 * HEAD_DIM]
    far = far_own[...]
    tails, heads = ends[0], ends[1]

    batch = 8
    for first in range(0, FAR_DILATION, batch):
        ats = [pl.ds(c * per, per) for c in range(first, first + batch)]
        units = []
        for at in ats:
            q = q_s[:, at, :].reshape(group * per, HEAD_DIM)
            kv = kv_s[:, at, :].reshape(group * per, 2 * HEAD_DIM)
            units.append((q, kv[:, :HEAD_DIM], kv[:, HEAD_DIM:], far))
        for at, found in zip(ats, softmax_parts(units)):
            for ref, value in zip(stats, found):
                ref[:, at, :] = value.reshape(group, per, HEAD_DIM)

    for b in range(group):
        if b == 0:
            slots, columns = (b, b + 1), slice(0, 2 * part)
        elif b == group - 1:
            slots, columns = (b - 1, b), slice(2 * part, 4 * part)
        else:
            slots, columns = (b, b + 1, b - 1), slice(0, 3 * part)
        units, places = [], []
        for residue in range(MIDDLE_DILATION):
            ats = residue_rows(residue, per)
            q = jnp.concatenate([q_s[b, at, :] for at in ats], axis=0)
            kv = jnp.concatenate([kv_s[j, at, :] for j in slots for at in ats], axis=0)
            units.append((q, kv[:, :HEAD_DIM], kv[:, HEAD_DIM:], middle_own[:, columns]))
            places.append(ats)
        for ats, found in zip(places, softmax_parts(units)):
            old = [jnp.concatenate([ref[b, at, :] for at in ats], axis=0) for ref in stats]
            for ref, value in zip(stats, join(old, found)):
                for s, at in enumerate(ats):
                    ref[b, at, :] = value[s * per : (s + 1) * per]

    half = rows // 2
    for b in range(group):
        pieces = [kv_s[b]]
        if b > 0:
            pieces.append(dot(tails, kv_s[b - 1]).astype(jnp.bfloat16))
        if b < group - 1:
            pieces.append(dot(heads, kv_s[b + 1]).astype(jnp.bfloat16))
        kv = jnp.concatenate(pieces, axis=0)
        low = rows if b > 0 else rows + side
        bias = jnp.concatenate([bias1[:, :rows], bias1[:, low : low + kv.shape[0] - rows]], axis=1)
        units = [
            (q_s[b, pl.ds(p * half, half), :], kv[:, :HEAD_DIM], kv[:, HEAD_DIM:], bias[p * half : (p + 1) * half])
            for p in range(2)
        ]
        for p, found in enumerate(softmax_parts(units)):
            at = pl.ds(p * half, half)
            for ref, value in zip(stats, join([ref[b, at, :] for ref in stats], found)):
                ref[b, at, :] = value


def by_member(refs):
    pieces = {}
    for members, ref in zip(PARCELS, refs):
        for j, k in enumerate(members):
            rows = ref.shape[0] // len(members)
            pieces[k] = ref.at[pl.ds(j * rows, rows)]
    return [pieces[k] for k in sorted(pieces)]


def halo_kernel(group, *refs):
    q_s, num_in, den_in, top_in = refs[:4]
    parcels = len(PARCELS)
    even_in, odd_in = by_member(refs[4 : 4 + parcels]), by_member(refs[4 + parcels : 4 + 2 * parcels])
    far_halo, touch_halo, ends = refs[4 + 2 * parcels : 7 + 2 * parcels]
    outs = refs[7 + 2 * parcels : 7 + 2 * parcels + group]
    num_s, den_s, top_s, touch, out_s = refs[7 + 2 * parcels + group :]
    rows = q_s.shape[1]
    per = rows // FAR_DILATION
    here = lax.axis_index("sp")
    me, mine = lax.rem(here, group), here // group
    even = lax.rem(mine, 2) == 0
    stats_in, stats = (num_in, den_in, top_in), (num_s, den_s, top_s)

    for slot, k, from_even in ((0, me ^ (group - 1), ~even), (1, me, even)):
        for wanted, pieces in ((from_even, even_in), (~from_even, odd_in)):
            for j, piece in enumerate(pieces):

                @pl.when(wanted & (k == j))
                def _():
                    touch[slot] = piece[...]

    steps = group * per
    far = far_halo[...]
    natural = token_order(rows).astype(jnp.bfloat16)
    tail = dot(ends[0], touch[0]).astype(jnp.bfloat16)
    head = dot(ends[1], touch[1]).astype(jnp.bfloat16)
    units, places = [], []
    for b, slot, beside in ((0, 0, tail), (group - 1, 1, head)):
        for residue in range(MIDDLE_DILATION):
            ats = residue_rows(residue, per)
            q = jnp.concatenate([q_s[b, at, :] for at in ats], axis=0)
            kv = jnp.concatenate([touch[slot, at, :] for at in ats] + [beside], axis=0)
            units.append((q, kv[:, :HEAD_DIM], kv[:, HEAD_DIM:], touch_halo[slot, residue]))
            places.append((b, ats))
    for (b, ats), found in zip(places, softmax_parts(units)):
        old = [jnp.concatenate([ref[b, at, :] for at in ats], axis=0) for ref in stats_in]
        for ref, value in zip(stats, join(old, found)):
            for s, at in enumerate(ats):
                ref[b // (group - 1), at, :] = value[s * per : (s + 1) * per]

    def old_of(joined, found, at):
        blocks = [joined[0, at, :]] + [found[b, at, :] for b in range(1, group - 1)] + [joined[1, at, :]]
        return jnp.concatenate(blocks, axis=0)

    batch = 8
    for first in range(0, FAR_DILATION, batch):
        ats = [pl.ds(c * per, per) for c in range(first, first + batch)]
        units = []
        for at in ats:
            q = q_s[:, at, :].reshape(steps, HEAD_DIM)
            kv = jnp.concatenate([piece[at, :] for piece in even_in + odd_in], axis=0)
            units.append((q, kv[:, :HEAD_DIM], kv[:, HEAD_DIM:], far))
        for at, found in zip(ats, softmax_parts(units)):
            num, den, _ = join([old_of(a, b, at) for a, b in zip(stats, stats_in)], found)
            out_s[:, at, :] = (num / den).astype(jnp.bfloat16).reshape(group, per, HEAD_DIM)
    for k in range(group):
        outs[k][...] = dot(natural, out_s[me ^ k]).astype(jnp.bfloat16)


def attend_local(group, q, own, own_masks):
    rows = own[0].shape[0]
    f32, bf16 = jnp.float32, jnp.bfloat16
    shape = (group, rows, HEAD_DIM)
    return pl.pallas_call(
        functools.partial(local_kernel, group),
        out_shape=[jax.ShapeDtypeStruct(shape, kind) for kind in (bf16, f32, f32, f32)],
        in_specs=[pl.BlockSpec(memory_space=pltpu.VMEM)] * (group + len(q) + 4),
        out_specs=[pl.BlockSpec(memory_space=pltpu.VMEM)] * 4,
        scratch_shapes=[pltpu.VMEM((group, rows, 2 * HEAD_DIM), bf16)],
        compiler_params=pltpu.CompilerParams(vmem_limit_bytes=VMEM_LIMIT),
        cost_estimate=pl.CostEstimate(flops=LOCAL_FLOPS, bytes_accessed=10**6, transcendentals=0),
    )(*own, *q.values(), *own_masks)


def attend_halo(group, found, even, odd, halo_masks):
    rows = found[0].shape[1]
    f32, bf16 = jnp.float32, jnp.bfloat16
    return pl.pallas_call(
        functools.partial(halo_kernel, group),
        out_shape=[jax.ShapeDtypeStruct((rows, HEAD_DIM), bf16)] * group,
        in_specs=[pl.BlockSpec(memory_space=pltpu.VMEM)] * (7 + len(even) + len(odd)),
        out_specs=[pl.BlockSpec(memory_space=pltpu.VMEM)] * group,
        scratch_shapes=[pltpu.VMEM((2, rows, HEAD_DIM), f32)] * 3
        + [
            pltpu.VMEM((2, rows, 2 * HEAD_DIM), bf16),
            pltpu.VMEM((group, rows, HEAD_DIM), bf16),
        ],
        compiler_params=pltpu.CompilerParams(vmem_limit_bytes=VMEM_LIMIT),
        cost_estimate=pl.CostEstimate(flops=10**9, bytes_accessed=10**6, transcendentals=0),
    )(*found, *even, *odd, *halo_masks)


def weight_rows(w_ref, group, k, columns):
    me, core = lax.rem(lax.axis_index("sp"), group), lax.axis_index("tp")
    rows = [(c * group + (me ^ k)) * HEAD_DIM for c in (core, 1 - core)]
    rows = [pl.ds(pl.multiple_of(row, HEAD_DIM), HEAD_DIM) for row in rows]
    return jnp.concatenate([w_ref[row, columns] for row in rows], axis=0)


def project_kernel(group, members, *refs):
    pieces = refs[: 2 * len(members)]
    w_ref, total_ref, out_ref, tiles, sems = refs[2 * len(members) :]
    width = tiles.shape[2]
    copies = []
    lefts = [
        jnp.concatenate([pieces[j][...], pieces[len(members) + j][...]], axis=1)
        for j in range(len(members))
    ]
    for tile in range(tiles.shape[0]):
        columns = pl.ds(tile * width, width)
        total = total_ref[:, columns]
        for k, left in zip(members, lefts):
            total += dot(left, weight_rows(w_ref, group, k, columns))
        tiles[tile] = total.astype(jnp.bfloat16)
        copies.append(pltpu.make_async_copy(tiles.at[tile], out_ref.at[:, columns], sems.at[tile]))
        copies[-1].start()
    for copy in copies:
        copy.wait()


def early_kernel(group, members, *refs):
    pieces = refs[: 2 * len(members)]
    w_ref, total_ref = refs[2 * len(members) :]
    total = None
    for j, k in enumerate(members):
        left = jnp.concatenate([pieces[j][...], pieces[len(members) + j][...]], axis=1)
        term = dot(left, weight_rows(w_ref, group, k, slice(None)))
        total = term if total is None else total + term
    total_ref[...] = total


def project_early(group, members, own, other, w_out):
    return pl.pallas_call(
        functools.partial(early_kernel, group, members),
        out_shape=jax.ShapeDtypeStruct((own[0].shape[0], w_out.shape[1]), jnp.float32),
        in_specs=[pl.BlockSpec(memory_space=pltpu.VMEM)] * (2 * len(members) + 1),
        out_specs=pl.BlockSpec(memory_space=pltpu.VMEM),
        compiler_params=pltpu.CompilerParams(vmem_limit_bytes=VMEM_LIMIT),
        cost_estimate=pl.CostEstimate(flops=10**6, bytes_accessed=10**6, transcendentals=0),
    )(*[x[k] for x in (own, other) for k in members], w_out)


def project(group, members, own, other, w_out, total):
    rows, width = own[0].shape[0], w_out.shape[1]
    tile = 256
    return pl.pallas_call(
        functools.partial(project_kernel, group, members),
        out_shape=jax.ShapeDtypeStruct((rows, width), jnp.bfloat16),
        in_specs=[pl.BlockSpec(memory_space=pltpu.VMEM)] * (2 * len(members) + 2),
        out_specs=pl.BlockSpec(memory_space=pl.ANY),
        scratch_shapes=[
            pltpu.VMEM((width // tile, rows, tile), jnp.bfloat16),
            pltpu.SemaphoreType.DMA((width // tile,)),
        ],
        compiler_params=pltpu.CompilerParams(vmem_limit_bytes=VMEM_LIMIT),
        cost_estimate=pl.CostEstimate(flops=10**9, bytes_accessed=10**6, transcendentals=0),
    )(*[x[k] for x in (own, other) for k in members], w_out, total)


def per_device(queries, keys, values, w_out):
    rows = queries.shape[0]
    shards = lax.axis_size("sp")
    group = -(-(SIDE_KEY_COUNT * FAR_DILATION) // rows)
    groups = shards // group

    def inside(value, k):
        return lax.ppermute(value, "sp", [(s, s ^ k) for s in range(shards)])

    def across(value, parity):
        pairs = []
        for s in range(shards):
            mine = s // group
            beside = mine + 1 if mine % 2 == parity else mine - 1
            for t in range(2):
                if 0 <= beside < groups:
                    pairs.append((2 * s + t, 2 * (s + (beside - mine) * group) + t))
                else:
                    pairs.append((2 * s + t, 2 * s + 1 - t))
        return lax.ppermute(value, ("sp", "tp"), pairs)

    def other_core(value):
        return lax.ppermute(value, "tp", [(0, 1), (1, 0)])

    kv, q = spread(group, keys, values, queries)
    own = [kv[0]] + [inside(kv[k], k) for k in range(1, group)]
    q = {k: inside(q[k], k) if k else q[k] for k in q}
    parcels = [pile([own[k] for k in members]) for members in PARCELS]
    even = [across(parcel, 0) for parcel in parcels]
    odd = [across(parcel, 1) for parcel in parcels]
    far_own, middle_own, near_own, far_halo, touch_halo, ends = masks(group, groups, rows)
    found = attend_local(group, q, own, (far_own, middle_own, near_own, ends))
    out = attend_halo(group, found, even, odd, (far_halo, touch_halo, ends))
    out = [out[0]] + [inside(out[k], k) for k in range(1, group)]
    swapped = [other_core(piece) for piece in out]
    total = project_early(group, EARLY, out, swapped, w_out)
    late = [k for k in range(group) if k not in EARLY]
    return project(group, late, out, swapped, w_out, total)


PARCELS = ((0,), (1, 2), (3,))
MERGED = (3,)
EARLY = (0, 1)


def solution(mesh):
    in_specs = (P("sp", "tp"), P("sp", "tp"), P("sp", "tp"), P(None, "tp"))
    out_specs = P("sp", "tp")
    return jax.shard_map(
        per_device, mesh=mesh, in_specs=in_specs, out_specs=out_specs, check_vma=False
    )
```

```python
import functools

import jax
import jax.numpy as jnp
from jax import lax
from jax.experimental import pallas as pl
from jax.experimental.pallas import tpu as pltpu
from jax.sharding import PartitionSpec as P


HEAD_DIM = 128
SIDE_KEY_COUNT = 64
MIDDLE_DILATION = 4
FAR_DILATION = 16
NEG = -1e30
COPY_PARTS = 1
NEAR_ROWS = 128
LOCAL_AHEAD = 12
HALO_AHEAD = 24
VMEM_LIMIT = 16 * 2**20
SPREAD_VMEM_LIMIT = 53 * 2**20
LOCAL_FLOPS = 2 * 10**9
LOG2E = 1.4426950408889634
EXP_SCALE = HEAD_DIM ** (-0.5) * LOG2E


def iota(shape, dim):
    return lax.broadcasted_iota(jnp.int32, shape, dim)


def class_major(rows):
    per = rows // FAR_DILATION
    out_row, in_row = iota((rows, rows), 0), iota((rows, rows), 1)
    return jnp.where(in_row == FAR_DILATION * (out_row % per) + out_row // per, 1.0, 0.0)


def token_order(rows):
    per = rows // FAR_DILATION
    out_row, in_row = iota((rows, rows), 0), iota((rows, rows), 1)
    return jnp.where(out_row == FAR_DILATION * (in_row % per) + in_row // per, 1.0, 0.0)


def dot(a, b):
    return jnp.dot(a, b, preferred_element_type=jnp.float32)


def dot_t(a, b):
    return lax.dot_general(a, b, (((1,), (1,)), ((), ())), preferred_element_type=jnp.float32)


def spread_kernel(group, *refs):
    ins, outs = refs[:3], refs[3:-4]
    keys, values, queries, sems = refs[-4:]
    kv_out, q_out = outs[:group], outs[group:]
    share = keys.shape[0] // COPY_PARTS
    parts = [pl.ds(p * share, share) for p in range(COPY_PARTS)]
    copies = [
        pltpu.make_async_copy(source.at[part], target.at[part], sems.at[j, p])
        for j, (source, target) in enumerate(zip(ins, (keys, values, queries)))
        for p, part in enumerate(parts)
    ]
    for copy in copies:
        copy.start()
    me = lax.rem(lax.axis_index("sp"), group)
    order = class_major(keys.shape[0]).astype(jnp.bfloat16)

    def columns(ref, k):
        return ref[:, pl.ds(pl.multiple_of((me ^ k) * HEAD_DIM, HEAD_DIM), HEAD_DIM)]

    for copy in copies[: 2 * COPY_PARTS]:
        copy.wait()
    for k in range(group):
        part = jnp.concatenate([columns(keys, k), columns(values, k)], axis=1)
        kv_out[k][:, : 2 * HEAD_DIM] = dot(order, part).astype(jnp.bfloat16)
    for copy in copies[2 * COPY_PARTS :]:
        copy.wait()
    q_out = iter(q_out)
    for k in range(group):
        part = dot(order, columns(queries, k)).astype(jnp.bfloat16)
        if k in MERGED:
            kv_out[k][:, 2 * HEAD_DIM :] = part
        else:
            next(q_out)[...] = part


def spread(group, keys, values, queries):
    rows = keys.shape[0]

    def shape(width):
        return jax.ShapeDtypeStruct((rows, width * HEAD_DIM), jnp.bfloat16)

    shapes = [shape(3 if k in MERGED else 2) for k in range(group)]
    shapes += [shape(1)] * (group - len(MERGED))
    found = pl.pallas_call(
        functools.partial(spread_kernel, group),
        out_shape=shapes,
        in_specs=[pl.BlockSpec(memory_space=pltpu.HBM)] * 3,
        out_specs=[pl.BlockSpec(memory_space=pltpu.VMEM)] * len(shapes),
        scratch_shapes=[pltpu.VMEM(keys.shape, jnp.bfloat16)] * 3 + [pltpu.SemaphoreType.DMA((3, COPY_PARTS))],
        compiler_params=pltpu.CompilerParams(vmem_limit_bytes=SPREAD_VMEM_LIMIT),
        cost_estimate=pl.CostEstimate(flops=10**6, bytes_accessed=10**6, transcendentals=0),
    )(keys, values, queries)
    return found[:group], dict(zip([k for k in range(group) if k not in MERGED], found[group:]))


def pile_kernel(*refs):
    rows, width = refs[0].shape[0], refs[-1].shape[1]
    for j, ref in enumerate(refs[:-1]):
        refs[-1][j * rows : (j + 1) * rows] = ref[:, :width]


def pile(pieces):
    if len(pieces) == 1 and pieces[0].shape[1] == 2 * HEAD_DIM:
        return pieces[0]
    rows = pieces[0].shape[0] * len(pieces)
    return pl.pallas_call(
        pile_kernel,
        out_shape=jax.ShapeDtypeStruct((rows, 2 * HEAD_DIM), pieces[0].dtype),
        in_specs=[pl.BlockSpec(memory_space=pltpu.VMEM)] * len(pieces),
        out_specs=pl.BlockSpec(memory_space=pltpu.VMEM),
        compiler_params=pltpu.CompilerParams(vmem_limit_bytes=VMEM_LIMIT),
        cost_estimate=pl.CostEstimate(flops=10**6, bytes_accessed=10**6, transcendentals=0),
    )(*pieces)


def middle_place(row, per):
    quarter = FAR_DILATION // MIDDLE_DILATION
    return quarter * (row % per) + (row // per) % quarter


def token_place(row, per):
    return FAR_DILATION * (row % per) + row // per


def band(q_pos, k_pos):
    return jnp.where(jnp.abs(k_pos - q_pos) <= SIDE_KEY_COUNT, 0.0, NEG)


def pick_tokens(rows, start, count):
    column = token_place(iota((count, rows), 1), rows // FAR_DILATION)
    return jnp.where(column == iota((count, rows), 0) + start, 1.0, 0.0).astype(jnp.bfloat16)


def residue_rows(residue, per):
    quarter = FAR_DILATION // MIDDLE_DILATION
    return [pl.ds((MIDDLE_DILATION * s + residue) * per, per) for s in range(quarter)]


def softmax_part(scores, values):
    top = jnp.max(scores, axis=1, keepdims=True)
    raised = jnp.exp2((scores - top) * EXP_SCALE).astype(jnp.bfloat16)
    both = dot(raised, jnp.concatenate([values, jnp.ones_like(values)], axis=1))
    num, den = both[:, :HEAD_DIM], both[:, HEAD_DIM:]
    return num, den, jnp.broadcast_to(top, num.shape)


def pipeline(units, ahead):
    pending = []
    for unit in list(units) + [None] * ahead:
        pending.append(unit and (unit[0](), unit))
        if len(pending) > ahead:
            done = pending.pop(0)
            if done:
                scores, (_, values, store) = done
                store(softmax_part(scores, values()))


def join(old, new):
    (num_a, den_a, top_a), (num_b, den_b, top_b) = old, new
    top = jnp.maximum(top_a, top_b)
    by_a, by_b = jnp.exp2((top_a - top) * EXP_SCALE), jnp.exp2((top_b - top) * EXP_SCALE)
    return num_a * by_a + num_b * by_b, den_a * by_a + den_b * by_b, top


def mask_kernel(group, groups, *refs):
    far_own, middle_own, near_own, far_halo, touch_halo, ends, natural = refs
    natural[...] = token_order(near_own.shape[0]).astype(jnp.bfloat16)
    rows = near_own.shape[0]
    per = rows // FAR_DILATION
    quarter = FAR_DILATION // MIDDLE_DILATION
    part = per * quarter
    side = SIDE_KEY_COUNT
    here = lax.axis_index("sp")
    me, mine = lax.rem(here, group), here // group
    even = lax.rem(mine, 2) == 0
    before = jnp.where(mine > 0, 0.0, NEG)
    after = jnp.where(mine < groups - 1, 0.0, NEG)

    steps = group * per
    far_own[...] = band(iota((steps, steps), 0), iota((steps, steps), 1))
    column = iota((part, 4 * part), 1)
    q_pos, k_pos = middle_place(iota((part, 4 * part), 0), per), middle_place(column, per)
    shard = jnp.where(column // part == 1, part, jnp.where(column // part == 2, -part, 0))
    middle_own[...] = band(q_pos, k_pos + shard)
    q_pos = token_place(iota((rows, rows), 0), per)
    near_own[:, :rows] = band(q_pos, token_place(iota((rows, rows), 1), per))
    q_pos, column = token_place(iota((rows, 2 * side), 0), per), iota((rows, 2 * side), 1)
    near_own[:, rows:] = band(q_pos, jnp.where(column < side, column - side, rows + column - side))

    column = iota((steps, 2 * steps), 1)
    place = ((column % steps) // per ^ me) * per + column % per
    behind = column // steps == jnp.where(even, 1, 0)
    k_pos = place + jnp.where(behind, -steps, steps)
    far_halo[...] = band(iota((steps, 2 * steps), 0), k_pos) + jnp.where(behind, before, after)
    q_mid, k_mid = middle_place(iota((part, part), 0), per), middle_place(iota((part, part), 1), per)
    row, token = iota((part, side), 0), iota((part, side), 1)
    for slot, (valid, step, start) in enumerate(((before, -part, -side), (after, part, rows))):
        for residue in range(MIDDLE_DILATION):
            q_pos = FAR_DILATION * (row % per) + MIDDLE_DILATION * (row // per) + residue
            touch_halo[slot, residue, :, :part] = band(q_mid, k_mid + step) + valid
            touch_halo[slot, residue, :, part:] = band(q_pos, token + start) + valid
    ends[0] = pick_tokens(rows, rows - side, side)
    ends[1] = pick_tokens(rows, 0, side)


def masks(group, groups, rows):
    per = rows // FAR_DILATION
    part = per * (FAR_DILATION // MIDDLE_DILATION)
    steps, side = group * per, SIDE_KEY_COUNT
    shapes = [
        (steps, steps),
        (part, 4 * part),
        (rows, rows + 2 * side),
        (steps, 2 * steps),
        (2, MIDDLE_DILATION, part, part + side),
    ]
    shapes = [jax.ShapeDtypeStruct(shape, jnp.float32) for shape in shapes]
    return pl.pallas_call(
        functools.partial(mask_kernel, group, groups),
        out_shape=shapes + [jax.ShapeDtypeStruct(s, jnp.bfloat16) for s in ((2, side, rows), (rows, rows))],
        out_specs=[pl.BlockSpec(memory_space=pltpu.VMEM)] * 7,
        compiler_params=pltpu.CompilerParams(vmem_limit_bytes=VMEM_LIMIT),
        cost_estimate=pl.CostEstimate(flops=10**6, bytes_accessed=10**6, transcendentals=0),
    )()


def local_kernel(group, *refs):
    kv_in, q_in, refs = refs[:group], refs[group:-9], refs[-9:]
    far_own, middle_own, bias1, ends, q_s, num_s, den_s, top_s, kv_s = refs
    rows = q_s.shape[1]
    per = rows // FAR_DILATION
    quarter = FAR_DILATION // MIDDLE_DILATION
    part = per * quarter
    side = SIDE_KEY_COUNT
    me = lax.rem(lax.axis_index("sp"), group)
    stats = (num_s, den_s, top_s)
    q_in = iter(q_in)
    for k in range(group):
        q_s[me ^ k] = kv_in[k][:, 2 * HEAD_DIM :] if k in MERGED else next(q_in)[...]
        kv_s[me ^ k] = kv_in[k][:, : 2 * HEAD_DIM]
    far = far_own[...]
    tails, heads = ends[0], ends[1]

    units = []

    def far_unit(c):
        at = pl.ds(c * per, per)

        def scores():
            q = q_s[:, at, :].reshape(group * per, HEAD_DIM)
            return dot_t(q, kv_s[:, at, :HEAD_DIM].reshape(group * per, HEAD_DIM)) + far

        def store(found):
            for ref, value in zip(stats, found):
                ref[:, at, :] = value.reshape(group, per, HEAD_DIM)

        return scores, lambda: kv_s[:, at, HEAD_DIM:].reshape(group * per, HEAD_DIM), store

    def middle_unit(b, residue):
        if b == 0:
            slots, columns = (b, b + 1), slice(0, 2 * part)
        elif b == group - 1:
            slots, columns = (b - 1, b), slice(2 * part, 4 * part)
        else:
            slots, columns = (b, b + 1, b - 1), slice(0, 3 * part)
        ats = residue_rows(residue, per)

        def keys(lanes):
            return jnp.concatenate([kv_s[j, at, lanes] for j in slots for at in ats], axis=0)

        def scores():
            q = jnp.concatenate([q_s[b, at, :] for at in ats], axis=0)
            return dot_t(q, keys(slice(0, HEAD_DIM))) + middle_own[:, columns]

        def store(found):
            old = [jnp.concatenate([ref[b, at, :] for at in ats], axis=0) for ref in stats]
            for ref, value in zip(stats, join(old, found)):
                for s, at in enumerate(ats):
                    ref[b, at, :] = value[s * per : (s + 1) * per]

        return scores, lambda: keys(slice(HEAD_DIM, 2 * HEAD_DIM)), store

    def near_units(b):
        pieces = [kv_s[b]]
        if b > 0:
            pieces.append(dot(tails, kv_s[b - 1]).astype(jnp.bfloat16))
        if b < group - 1:
            pieces.append(dot(heads, kv_s[b + 1]).astype(jnp.bfloat16))
        kv = jnp.concatenate(pieces, axis=0)
        low = rows if b > 0 else rows + side
        count = rows // NEAR_ROWS
        for p in range(count):
            at = pl.ds(p * NEAR_ROWS, NEAR_ROWS)

            def scores(at=at):
                outer = bias1[at, low : low + kv.shape[0] - rows]
                return dot_t(q_s[b, at, :], kv[:, :HEAD_DIM]) + jnp.concatenate([bias1[at, :rows], outer], axis=1)

            def store(found, at=at):
                for ref, value in zip(stats, join([ref[b, at, :] for ref in stats], found)):
                    ref[b, at, :] = value

            yield scores, lambda: kv[:, HEAD_DIM:], store

    units += [far_unit(c) for c in range(FAR_DILATION)]
    for b in range(group):
        units += [middle_unit(b, residue) for residue in range(MIDDLE_DILATION)]
    for b in range(group):
        units += near_units(b)
    pipeline(units, LOCAL_AHEAD)


def by_member(refs):
    pieces = {}
    for members, ref in zip(PARCELS, refs):
        for j, k in enumerate(members):
            rows = ref.shape[0] // len(members)
            pieces[k] = ref.at[pl.ds(j * rows, rows)]
    return [pieces[k] for k in sorted(pieces)]


def halo_kernel(group, *refs):
    q_s, num_in, den_in, top_in = refs[:4]
    parcels = len(PARCELS)
    even_in, odd_in = by_member(refs[4 : 4 + parcels]), by_member(refs[4 + parcels : 4 + 2 * parcels])
    far_halo, touch_halo, ends, natural = refs[4 + 2 * parcels : 8 + 2 * parcels]
    outs = refs[8 + 2 * parcels : 8 + 2 * parcels + group]
    num_s, den_s, top_s, touch, out_s = refs[8 + 2 * parcels + group :]
    rows = q_s.shape[1]
    per = rows // FAR_DILATION
    here = lax.axis_index("sp")
    me, mine = lax.rem(here, group), here // group
    even = lax.rem(mine, 2) == 0
    stats_in, stats = (num_in, den_in, top_in), (num_s, den_s, top_s)

    for slot, k, from_even in ((0, me ^ (group - 1), ~even), (1, me, even)):
        for wanted, pieces in ((from_even, even_in), (~from_even, odd_in)):
            for j, piece in enumerate(pieces):

                @pl.when(wanted & (k == j))
                def _():
                    touch[slot] = piece[...]

    steps = group * per
    far = far_halo[...]
    tail = dot(ends[0], touch[0]).astype(jnp.bfloat16)
    head = dot(ends[1], touch[1]).astype(jnp.bfloat16)

    def touch_unit(b, slot, beside, residue):
        ats = residue_rows(residue, per)
        kv = jnp.concatenate([touch[slot, at, :] for at in ats] + [beside], axis=0)

        def scores():
            q = jnp.concatenate([q_s[b, at, :] for at in ats], axis=0)
            return dot_t(q, kv[:, :HEAD_DIM]) + touch_halo[slot, residue]

        def store(found):
            old = [jnp.concatenate([ref[b, at, :] for at in ats], axis=0) for ref in stats_in]
            for ref, value in zip(stats, join(old, found)):
                for s, at in enumerate(ats):
                    ref[slot, at, :] = value[s * per : (s + 1) * per]

        return scores, lambda: kv[:, HEAD_DIM:], store

    def old_of(joined, found, at):
        blocks = [joined[0, at, :]] + [found[b, at, :] for b in range(1, group - 1)] + [joined[1, at, :]]
        return jnp.concatenate(blocks, axis=0)

    def far_unit(c):
        at = pl.ds(c * per, per)

        def keys(lanes):
            return jnp.concatenate([piece[at, lanes] for piece in even_in + odd_in], axis=0)

        def scores():
            return dot_t(q_s[:, at, :].reshape(steps, HEAD_DIM), keys(slice(0, HEAD_DIM))) + far

        def store(found):
            num, den, _ = join([old_of(a, b, at) for a, b in zip(stats, stats_in)], found)
            out_s[:, at, :] = (num / den).astype(jnp.bfloat16).reshape(group, per, HEAD_DIM)

        return scores, lambda: keys(slice(HEAD_DIM, 2 * HEAD_DIM)), store

    units = []
    for b, slot, beside in ((0, 0, tail), (group - 1, 1, head)):
        units += [touch_unit(b, slot, beside, residue) for residue in range(MIDDLE_DILATION)]
    units += [far_unit(c) for c in range(FAR_DILATION)]
    pipeline(units, HALO_AHEAD)
    for k in range(group):
        outs[k][...] = dot(natural[...], out_s[me ^ k]).astype(jnp.bfloat16)


def attend_local(group, q, own, own_masks):
    rows = own[0].shape[0]
    f32, bf16 = jnp.float32, jnp.bfloat16
    shape = (group, rows, HEAD_DIM)
    return pl.pallas_call(
        functools.partial(local_kernel, group),
        out_shape=[jax.ShapeDtypeStruct(shape, kind) for kind in (bf16, f32, f32, f32)],
        in_specs=[pl.BlockSpec(memory_space=pltpu.VMEM)] * (group + len(q) + 4),
        out_specs=[pl.BlockSpec(memory_space=pltpu.VMEM)] * 4,
        scratch_shapes=[pltpu.VMEM((group, rows, 2 * HEAD_DIM), bf16)],
        compiler_params=pltpu.CompilerParams(vmem_limit_bytes=VMEM_LIMIT),
        cost_estimate=pl.CostEstimate(flops=LOCAL_FLOPS, bytes_accessed=10**6, transcendentals=0),
    )(*own, *q.values(), *own_masks)


def attend_halo(group, found, even, odd, halo_masks):
    rows = found[0].shape[1]
    f32, bf16 = jnp.float32, jnp.bfloat16
    return pl.pallas_call(
        functools.partial(halo_kernel, group),
        out_shape=[jax.ShapeDtypeStruct((rows, HEAD_DIM), bf16)] * group,
        in_specs=[pl.BlockSpec(memory_space=pltpu.VMEM)] * (8 + len(even) + len(odd)),
        out_specs=[pl.BlockSpec(memory_space=pltpu.VMEM)] * group,
        scratch_shapes=[pltpu.VMEM((2, rows, HEAD_DIM), f32)] * 3
        + [
            pltpu.VMEM((2, rows, 2 * HEAD_DIM), bf16),
            pltpu.VMEM((group, rows, HEAD_DIM), bf16),
        ],
        compiler_params=pltpu.CompilerParams(vmem_limit_bytes=VMEM_LIMIT),
        cost_estimate=pl.CostEstimate(flops=10**9, bytes_accessed=10**6, transcendentals=0),
    )(*found, *even, *odd, *halo_masks)


def weight_rows(w_ref, group, k, columns):
    me, core = lax.rem(lax.axis_index("sp"), group), lax.axis_index("tp")
    rows = [(c * group + (me ^ k)) * HEAD_DIM for c in (core, 1 - core)]
    rows = [pl.ds(pl.multiple_of(row, HEAD_DIM), HEAD_DIM) for row in rows]
    return jnp.concatenate([w_ref[row, columns] for row in rows], axis=0)


def project_kernel(group, members, *refs):
    pieces = refs[: 2 * len(members)]
    w_ref, total_ref, out_ref, tiles, sems = refs[2 * len(members) :]
    width = tiles.shape[2]
    copies = []
    lefts = [
        jnp.concatenate([pieces[j][...], pieces[len(members) + j][...]], axis=1)
        for j in range(len(members))
    ]
    for tile in range(tiles.shape[0]):
        columns = pl.ds(tile * width, width)
        total = total_ref[:, columns]
        for k, left in zip(members, lefts):
            total += dot(left, weight_rows(w_ref, group, k, columns))
        tiles[tile] = total.astype(jnp.bfloat16)
        copies.append(pltpu.make_async_copy(tiles.at[tile], out_ref.at[:, columns], sems.at[tile]))
        copies[-1].start()
    for copy in copies:
        copy.wait()


def early_kernel(group, members, *refs):
    pieces = refs[: 2 * len(members)]
    w_ref, total_ref = refs[2 * len(members) :]
    total = None
    for j, k in enumerate(members):
        left = jnp.concatenate([pieces[j][...], pieces[len(members) + j][...]], axis=1)
        term = dot(left, weight_rows(w_ref, group, k, slice(None)))
        total = term if total is None else total + term
    total_ref[...] = total


def project_early(group, members, own, other, w_out):
    return pl.pallas_call(
        functools.partial(early_kernel, group, members),
        out_shape=jax.ShapeDtypeStruct((own[0].shape[0], w_out.shape[1]), jnp.float32),
        in_specs=[pl.BlockSpec(memory_space=pltpu.VMEM)] * (2 * len(members) + 1),
        out_specs=pl.BlockSpec(memory_space=pltpu.VMEM),
        compiler_params=pltpu.CompilerParams(vmem_limit_bytes=VMEM_LIMIT),
        cost_estimate=pl.CostEstimate(flops=10**6, bytes_accessed=10**6, transcendentals=0),
    )(*[x[k] for x in (own, other) for k in members], w_out)


def project(group, members, own, other, w_out, total):
    rows, width = own[0].shape[0], w_out.shape[1]
    tile = 256
    return pl.pallas_call(
        functools.partial(project_kernel, group, members),
        out_shape=jax.ShapeDtypeStruct((rows, width), jnp.bfloat16),
        in_specs=[pl.BlockSpec(memory_space=pltpu.VMEM)] * (2 * len(members) + 2),
        out_specs=pl.BlockSpec(memory_space=pl.ANY),
        scratch_shapes=[
            pltpu.VMEM((width // tile, rows, tile), jnp.bfloat16),
            pltpu.SemaphoreType.DMA((width // tile,)),
        ],
        compiler_params=pltpu.CompilerParams(vmem_limit_bytes=VMEM_LIMIT),
        cost_estimate=pl.CostEstimate(flops=10**9, bytes_accessed=10**6, transcendentals=0),
    )(*[x[k] for x in (own, other) for k in members], w_out, total)


def per_device(queries, keys, values, w_out):
    rows = queries.shape[0]
    shards = lax.axis_size("sp")
    group = -(-(SIDE_KEY_COUNT * FAR_DILATION) // rows)
    groups = shards // group

    def inside(value, k):
        return lax.ppermute(value, "sp", [(s, s ^ k) for s in range(shards)])

    def across(value, parity):
        pairs = []
        for s in range(shards):
            mine = s // group
            beside = mine + 1 if mine % 2 == parity else mine - 1
            for t in range(2):
                if 0 <= beside < groups:
                    pairs.append((2 * s + t, 2 * (s + (beside - mine) * group) + t))
                else:
                    pairs.append((2 * s + t, 2 * s + 1 - t))
        return lax.ppermute(value, ("sp", "tp"), pairs)

    def other_core(value):
        return lax.ppermute(value, "tp", [(0, 1), (1, 0)])

    kv, q = spread(group, keys, values, queries)
    own = [kv[0]] + [inside(kv[k], k) for k in range(1, group)]
    q = {k: inside(q[k], k) if k else q[k] for k in q}
    parcels = [pile([own[k] for k in members]) for members in PARCELS]
    even = [across(parcel, 0) for parcel in parcels]
    odd = [across(parcel, 1) for parcel in parcels]
    far_own, middle_own, near_own, far_halo, touch_halo, ends, natural = masks(group, groups, rows)
    found = attend_local(group, q, own, (far_own, middle_own, near_own, ends))
    out = attend_halo(group, found, even, odd, (far_halo, touch_halo, ends, natural))
    out = [out[0]] + [inside(out[k], k) for k in range(1, group)]
    swapped = [other_core(piece) for piece in out]
    total = project_early(group, EARLY, out, swapped, w_out)
    late = [k for k in range(group) if k not in EARLY]
    return project(group, late, out, swapped, w_out, total)


PARCELS = ((0,), (1, 2), (3,))
MERGED = (3,)
EARLY = (0, 1)


def solution(mesh):
    in_specs = (P("sp", "tp"), P("sp", "tp"), P("sp", "tp"), P(None, "tp"))
    out_specs = P("sp", "tp")
    return jax.shard_map(
        per_device, mesh=mesh, in_specs=in_specs, out_specs=out_specs, check_vma=False
    )
```

```python
import functools

import jax
import jax.numpy as jnp
from jax import lax
from jax.experimental import pallas as pl
from jax.experimental.pallas import tpu as pltpu
from jax.sharding import PartitionSpec as P


HEAD_DIM = 128
SIDE_KEY_COUNT = 64
MIDDLE_DILATION = 4
FAR_DILATION = 16
NEG = -1e30
COPY_PARTS = 1
NEAR_ROWS = 128
LOCAL_AHEAD = 12
HALO_AHEAD = 24
VMEM_LIMIT = 16 * 2**20
SPREAD_VMEM_LIMIT = 53 * 2**20
LOCAL_FLOPS = 2 * 10**9
LOG2E = 1.4426950408889634
EXP_SCALE = HEAD_DIM ** (-0.5) * LOG2E


def iota(shape, dim):
    return lax.broadcasted_iota(jnp.int32, shape, dim)


def class_major(rows):
    per = rows // FAR_DILATION
    out_row, in_row = iota((rows, rows), 0), iota((rows, rows), 1)
    return jnp.where(in_row == FAR_DILATION * (out_row % per) + out_row // per, 1.0, 0.0)


def token_order(rows):
    per = rows // FAR_DILATION
    out_row, in_row = iota((rows, rows), 0), iota((rows, rows), 1)
    return jnp.where(out_row == FAR_DILATION * (in_row % per) + in_row // per, 1.0, 0.0)


def dot(a, b):
    return jnp.dot(a, b, preferred_element_type=jnp.float32)


def dot_t(a, b):
    return lax.dot_general(a, b, (((1,), (1,)), ((), ())), preferred_element_type=jnp.float32)


def spread_kernel(group, *refs):
    ins, outs = refs[:3], refs[3:-4]
    keys, values, queries, sems = refs[-4:]
    kv_out, q_out = outs[:group], outs[group:]
    share = keys.shape[0] // COPY_PARTS
    parts = [pl.ds(p * share, share) for p in range(COPY_PARTS)]
    copies = [
        pltpu.make_async_copy(source.at[part], target.at[part], sems.at[j, p])
        for j, (source, target) in enumerate(zip(ins, (keys, values, queries)))
        for p, part in enumerate(parts)
    ]
    for copy in copies:
        copy.start()
    me = lax.rem(lax.axis_index("sp"), group)
    order = class_major(keys.shape[0]).astype(jnp.bfloat16)

    def columns(ref, k):
        return ref[:, pl.ds(pl.multiple_of((me ^ k) * HEAD_DIM, HEAD_DIM), HEAD_DIM)]

    for copy in copies[: 2 * COPY_PARTS]:
        copy.wait()
    for k in range(group):
        part = jnp.concatenate([columns(keys, k), columns(values, k)], axis=1)
        kv_out[k][:, : 2 * HEAD_DIM] = dot(order, part).astype(jnp.bfloat16)
    for copy in copies[2 * COPY_PARTS :]:
        copy.wait()
    q_out = iter(q_out)
    for k in range(group):
        part = dot(order, columns(queries, k)).astype(jnp.bfloat16)
        if k in MERGED:
            kv_out[k][:, 2 * HEAD_DIM :] = part
        else:
            next(q_out)[...] = part


def spread(group, keys, values, queries):
    rows = keys.shape[0]

    def shape(width):
        return jax.ShapeDtypeStruct((rows, width * HEAD_DIM), jnp.bfloat16)

    shapes = [shape(3 if k in MERGED else 2) for k in range(group)]
    shapes += [shape(1)] * (group - len(MERGED))
    found = pl.pallas_call(
        functools.partial(spread_kernel, group),
        out_shape=shapes,
        in_specs=[pl.BlockSpec(memory_space=pltpu.HBM)] * 3,
        out_specs=[pl.BlockSpec(memory_space=pltpu.VMEM)] * len(shapes),
        scratch_shapes=[pltpu.VMEM(keys.shape, jnp.bfloat16)] * 3 + [pltpu.SemaphoreType.DMA((3, COPY_PARTS))],
        compiler_params=pltpu.CompilerParams(vmem_limit_bytes=SPREAD_VMEM_LIMIT),
        cost_estimate=pl.CostEstimate(flops=10**6, bytes_accessed=10**6, transcendentals=0),
    )(keys, values, queries)
    return found[:group], dict(zip([k for k in range(group) if k not in MERGED], found[group:]))


def pile_kernel(*refs):
    rows, width = refs[0].shape[0], refs[-1].shape[1]
    for j, ref in enumerate(refs[:-1]):
        refs[-1][j * rows : (j + 1) * rows] = ref[:, :width]


def pile(pieces):
    if len(pieces) == 1 and pieces[0].shape[1] == 2 * HEAD_DIM:
        return pieces[0]
    rows = pieces[0].shape[0] * len(pieces)
    return pl.pallas_call(
        pile_kernel,
        out_shape=jax.ShapeDtypeStruct((rows, 2 * HEAD_DIM), pieces[0].dtype),
        in_specs=[pl.BlockSpec(memory_space=pltpu.VMEM)] * len(pieces),
        out_specs=pl.BlockSpec(memory_space=pltpu.VMEM),
        compiler_params=pltpu.CompilerParams(vmem_limit_bytes=VMEM_LIMIT),
        cost_estimate=pl.CostEstimate(flops=10**6, bytes_accessed=10**6, transcendentals=0),
    )(*pieces)


def middle_place(row, per):
    quarter = FAR_DILATION // MIDDLE_DILATION
    return quarter * (row % per) + (row // per) % quarter


def token_place(row, per):
    return FAR_DILATION * (row % per) + row // per


def band(q_pos, k_pos):
    return jnp.where(jnp.abs(k_pos - q_pos) <= SIDE_KEY_COUNT, 0.0, NEG)


def pick_tokens(rows, start, count):
    column = token_place(iota((count, rows), 1), rows // FAR_DILATION)
    return jnp.where(column == iota((count, rows), 0) + start, 1.0, 0.0).astype(jnp.bfloat16)


def residue_rows(residue, per):
    quarter = FAR_DILATION // MIDDLE_DILATION
    return [pl.ds((MIDDLE_DILATION * s + residue) * per, per) for s in range(quarter)]


def softmax_part(scores, values):
    top = jnp.max(scores, axis=1, keepdims=True)
    raised = jnp.exp2((scores - top) * EXP_SCALE).astype(jnp.bfloat16)
    both = dot(raised, jnp.concatenate([values, jnp.ones_like(values)], axis=1))
    num, den = both[:, :HEAD_DIM], both[:, HEAD_DIM:]
    return num, den, jnp.broadcast_to(top, num.shape)


def pipeline(units, ahead):
    pending = []
    for unit in list(units) + [None] * ahead:
        pending.append(unit and (unit[0](), unit))
        if len(pending) > ahead:
            done = pending.pop(0)
            if done:
                scores, (_, values, store) = done
                store(softmax_part(scores, values()))


def join(old, new):
    (num_a, den_a, top_a), (num_b, den_b, top_b) = old, new
    top = jnp.maximum(top_a, top_b)
    by_a, by_b = jnp.exp2((top_a - top) * EXP_SCALE), jnp.exp2((top_b - top) * EXP_SCALE)
    return num_a * by_a + num_b * by_b, den_a * by_a + den_b * by_b, top


def mask_kernel(group, groups, *refs):
    far_own, middle_own, near_own, far_halo, touch_halo, ends, natural = refs
    natural[...] = token_order(near_own.shape[0]).astype(jnp.bfloat16)
    rows = near_own.shape[0]
    per = rows // FAR_DILATION
    quarter = FAR_DILATION // MIDDLE_DILATION
    part = per * quarter
    side = SIDE_KEY_COUNT
    here = lax.axis_index("sp")
    me, mine = lax.rem(here, group), here // group
    even = lax.rem(mine, 2) == 0
    before = jnp.where(mine > 0, 0.0, NEG)
    after = jnp.where(mine < groups - 1, 0.0, NEG)

    steps = group * per
    far_own[...] = band(iota((steps, steps), 0), iota((steps, steps), 1))
    column = iota((part, 4 * part), 1)
    q_pos, k_pos = middle_place(iota((part, 4 * part), 0), per), middle_place(column, per)
    shard = jnp.where(column // part == 1, part, jnp.where(column // part == 2, -part, 0))
    middle_own[...] = band(q_pos, k_pos + shard)
    q_pos = token_place(iota((rows, rows), 0), per)
    near_own[:, :rows] = band(q_pos, token_place(iota((rows, rows), 1), per))
    q_pos, column = token_place(iota((rows, 2 * side), 0), per), iota((rows, 2 * side), 1)
    near_own[:, rows:] = band(q_pos, jnp.where(column < side, column - side, rows + column - side))

    column = iota((steps, 2 * steps), 1)
    place = ((column % steps) // per ^ me) * per + column % per
    behind = column // steps == jnp.where(even, 1, 0)
    k_pos = place + jnp.where(behind, -steps, steps)
    far_halo[...] = band(iota((steps, 2 * steps), 0), k_pos) + jnp.where(behind, before, after)
    q_mid, k_mid = middle_place(iota((part, part), 0), per), middle_place(iota((part, part), 1), per)
    row, token = iota((part, side), 0), iota((part, side), 1)
    for slot, (valid, step, start) in enumerate(((before, -part, -side), (after, part, rows))):
        for residue in range(MIDDLE_DILATION):
            q_pos = FAR_DILATION * (row % per) + MIDDLE_DILATION * (row // per) + residue
            touch_halo[slot, residue, :, :part] = band(q_mid, k_mid + step) + valid
            touch_halo[slot, residue, :, part:] = band(q_pos, token + start) + valid
    ends[0] = pick_tokens(rows, rows - side, side)
    ends[1] = pick_tokens(rows, 0, side)


def masks(group, groups, rows):
    per = rows // FAR_DILATION
    part = per * (FAR_DILATION // MIDDLE_DILATION)
    steps, side = group * per, SIDE_KEY_COUNT
    shapes = [
        (steps, steps),
        (part, 4 * part),
        (rows, rows + 2 * side),
        (steps, 2 * steps),
        (2, MIDDLE_DILATION, part, part + side),
    ]
    shapes = [jax.ShapeDtypeStruct(shape, jnp.float32) for shape in shapes]
    return pl.pallas_call(
        functools.partial(mask_kernel, group, groups),
        out_shape=shapes + [jax.ShapeDtypeStruct(s, jnp.bfloat16) for s in ((2, side, rows), (rows, rows))],
        out_specs=[pl.BlockSpec(memory_space=pltpu.VMEM)] * 7,
        compiler_params=pltpu.CompilerParams(vmem_limit_bytes=VMEM_LIMIT),
        cost_estimate=pl.CostEstimate(flops=10**6, bytes_accessed=10**6, transcendentals=0),
    )()


def local_kernel(group, *refs):
    kv_in, q_in, refs = refs[:group], refs[group:-9], refs[-9:]
    far_own, middle_own, bias1, ends, q_s, num_s, den_s, top_s, kv_s = refs
    rows = q_s.shape[1]
    per = rows // FAR_DILATION
    quarter = FAR_DILATION // MIDDLE_DILATION
    part = per * quarter
    side = SIDE_KEY_COUNT
    me = lax.rem(lax.axis_index("sp"), group)
    stats = (num_s, den_s, top_s)
    q_in = iter(q_in)
    for k in range(group):
        q_s[me ^ k] = kv_in[k][:, 2 * HEAD_DIM :] if k in MERGED else next(q_in)[...]
        kv_s[me ^ k] = kv_in[k][:, : 2 * HEAD_DIM]
    far = far_own[...]
    tails, heads = ends[0], ends[1]

    units = []

    def far_unit(c):
        at = pl.ds(c * per, per)

        def scores():
            q = q_s[:, at, :].reshape(group * per, HEAD_DIM)
            return dot_t(q, kv_s[:, at, :HEAD_DIM].reshape(group * per, HEAD_DIM)) + far

        def store(found):
            for ref, value in zip(stats, found):
                ref[:, at, :] = value.reshape(group, per, HEAD_DIM)

        return scores, lambda: kv_s[:, at, HEAD_DIM:].reshape(group * per, HEAD_DIM), store

    def middle_unit(b, residue):
        if b == 0:
            slots, columns = (b, b + 1), slice(0, 2 * part)
        elif b == group - 1:
            slots, columns = (b - 1, b), slice(2 * part, 4 * part)
        else:
            slots, columns = (b, b + 1, b - 1), slice(0, 3 * part)
        ats = residue_rows(residue, per)

        def keys(lanes):
            return jnp.concatenate([kv_s[j, at, lanes] for j in slots for at in ats], axis=0)

        def scores():
            q = jnp.concatenate([q_s[b, at, :] for at in ats], axis=0)
            return dot_t(q, keys(slice(0, HEAD_DIM))) + middle_own[:, columns]

        def store(found):
            old = [jnp.concatenate([ref[b, at, :] for at in ats], axis=0) for ref in stats]
            for ref, value in zip(stats, join(old, found)):
                for s, at in enumerate(ats):
                    ref[b, at, :] = value[s * per : (s + 1) * per]

        return scores, lambda: keys(slice(HEAD_DIM, 2 * HEAD_DIM)), store

    def near_units(b):
        pieces = [kv_s[b]]
        if b > 0:
            pieces.append(dot(tails, kv_s[b - 1]).astype(jnp.bfloat16))
        if b < group - 1:
            pieces.append(dot(heads, kv_s[b + 1]).astype(jnp.bfloat16))
        kv = jnp.concatenate(pieces, axis=0)
        low = rows if b > 0 else rows + side
        count = rows // NEAR_ROWS
        for p in range(count):
            at = pl.ds(p * NEAR_ROWS, NEAR_ROWS)

            def scores(at=at):
                outer = bias1[at, low : low + kv.shape[0] - rows]
                return dot_t(q_s[b, at, :], kv[:, :HEAD_DIM]) + jnp.concatenate([bias1[at, :rows], outer], axis=1)

            def store(found, at=at):
                for ref, value in zip(stats, join([ref[b, at, :] for ref in stats], found)):
                    ref[b, at, :] = value

            yield scores, lambda: kv[:, HEAD_DIM:], store

    units += [far_unit(c) for c in range(FAR_DILATION)]
    for b in range(group):
        units += [middle_unit(b, residue) for residue in range(MIDDLE_DILATION)]
    for b in range(group):
        units += near_units(b)
    pipeline(units, LOCAL_AHEAD)


def by_member(refs):
    pieces = {}
    for members, ref in zip(PARCELS, refs):
        for j, k in enumerate(members):
            rows = ref.shape[0] // len(members)
            pieces[k] = ref.at[pl.ds(j * rows, rows)]
    return [pieces[k] for k in sorted(pieces)]


def halo_kernel(group, *refs):
    q_s, num_in, den_in, top_in = refs[:4]
    parcels = len(PARCELS)
    even_in, odd_in = by_member(refs[4 : 4 + parcels]), by_member(refs[4 + parcels : 4 + 2 * parcels])
    far_halo, touch_halo, ends, natural = refs[4 + 2 * parcels : 8 + 2 * parcels]
    outs = refs[8 + 2 * parcels : 8 + 2 * parcels + group]
    num_s, den_s, top_s, touch, out_s = refs[8 + 2 * parcels + group :]
    rows = q_s.shape[1]
    per = rows // FAR_DILATION
    here = lax.axis_index("sp")
    me, mine = lax.rem(here, group), here // group
    even = lax.rem(mine, 2) == 0
    stats_in, stats = (num_in, den_in, top_in), (num_s, den_s, top_s)

    for slot, k, from_even in ((0, me ^ (group - 1), ~even), (1, me, even)):
        for wanted, pieces in ((from_even, even_in), (~from_even, odd_in)):

            @pl.when(wanted)
            def _():
                for j, piece in enumerate(pieces):

                    @pl.when(k == j)
                    def _():
                        touch[slot] = piece[...]

    steps = group * per
    far = far_halo[...]
    tail = dot(ends[0], touch[0]).astype(jnp.bfloat16)
    head = dot(ends[1], touch[1]).astype(jnp.bfloat16)

    def touch_unit(b, slot, beside, residue):
        ats = residue_rows(residue, per)
        kv = jnp.concatenate([touch[slot, at, :] for at in ats] + [beside], axis=0)

        def scores():
            q = jnp.concatenate([q_s[b, at, :] for at in ats], axis=0)
            return dot_t(q, kv[:, :HEAD_DIM]) + touch_halo[slot, residue]

        def store(found):
            old = [jnp.concatenate([ref[b, at, :] for at in ats], axis=0) for ref in stats_in]
            for ref, value in zip(stats, join(old, found)):
                for s, at in enumerate(ats):
                    ref[slot, at, :] = value[s * per : (s + 1) * per]

        return scores, lambda: kv[:, HEAD_DIM:], store

    def old_of(joined, found, at):
        blocks = [joined[0, at, :]] + [found[b, at, :] for b in range(1, group - 1)] + [joined[1, at, :]]
        return jnp.concatenate(blocks, axis=0)

    def far_unit(c):
        at = pl.ds(c * per, per)

        def keys(lanes):
            return jnp.concatenate([piece[at, lanes] for piece in even_in + odd_in], axis=0)

        def scores():
            return dot_t(q_s[:, at, :].reshape(steps, HEAD_DIM), keys(slice(0, HEAD_DIM))) + far

        def store(found):
            num, den, _ = join([old_of(a, b, at) for a, b in zip(stats, stats_in)], found)
            out_s[:, at, :] = (num / den).astype(jnp.bfloat16).reshape(group, per, HEAD_DIM)

        return scores, lambda: keys(slice(HEAD_DIM, 2 * HEAD_DIM)), store

    units = []
    for b, slot, beside in ((0, 0, tail), (group - 1, 1, head)):
        units += [touch_unit(b, slot, beside, residue) for residue in range(MIDDLE_DILATION)]
    units += [far_unit(c) for c in range(FAR_DILATION)]
    pipeline(units, HALO_AHEAD)
    for k in range(group):
        outs[k][...] = dot(natural[...], out_s[me ^ k]).astype(jnp.bfloat16)


def attend_local(group, q, own, own_masks):
    rows = own[0].shape[0]
    f32, bf16 = jnp.float32, jnp.bfloat16
    shape = (group, rows, HEAD_DIM)
    return pl.pallas_call(
        functools.partial(local_kernel, group),
        out_shape=[jax.ShapeDtypeStruct(shape, kind) for kind in (bf16, f32, f32, f32)],
        in_specs=[pl.BlockSpec(memory_space=pltpu.VMEM)] * (group + len(q) + 4),
        out_specs=[pl.BlockSpec(memory_space=pltpu.VMEM)] * 4,
        scratch_shapes=[pltpu.VMEM((group, rows, 2 * HEAD_DIM), bf16)],
        compiler_params=pltpu.CompilerParams(vmem_limit_bytes=VMEM_LIMIT),
        cost_estimate=pl.CostEstimate(flops=LOCAL_FLOPS, bytes_accessed=10**6, transcendentals=0),
    )(*own, *q.values(), *own_masks)


def attend_halo(group, found, even, odd, halo_masks):
    rows = found[0].shape[1]
    f32, bf16 = jnp.float32, jnp.bfloat16
    return pl.pallas_call(
        functools.partial(halo_kernel, group),
        out_shape=[jax.ShapeDtypeStruct((rows, HEAD_DIM), bf16)] * group,
        in_specs=[pl.BlockSpec(memory_space=pltpu.VMEM)] * (8 + len(even) + len(odd)),
        out_specs=[pl.BlockSpec(memory_space=pltpu.VMEM)] * group,
        scratch_shapes=[pltpu.VMEM((2, rows, HEAD_DIM), f32)] * 3
        + [
            pltpu.VMEM((2, rows, 2 * HEAD_DIM), bf16),
            pltpu.VMEM((group, rows, HEAD_DIM), bf16),
        ],
        compiler_params=pltpu.CompilerParams(vmem_limit_bytes=VMEM_LIMIT),
        cost_estimate=pl.CostEstimate(flops=10**9, bytes_accessed=10**6, transcendentals=0),
    )(*found, *even, *odd, *halo_masks)


def weight_rows(w_ref, group, k, columns):
    me, core = lax.rem(lax.axis_index("sp"), group), lax.axis_index("tp")
    rows = [(c * group + (me ^ k)) * HEAD_DIM for c in (core, 1 - core)]
    rows = [pl.ds(pl.multiple_of(row, HEAD_DIM), HEAD_DIM) for row in rows]
    return jnp.concatenate([w_ref[row, columns] for row in rows], axis=0)


def project_kernel(group, members, *refs):
    pieces = refs[: 2 * len(members)]
    w_ref, total_ref, out_ref, tiles, sems = refs[2 * len(members) :]
    height = tiles.shape[1]
    copies = []
    lefts = [
        jnp.concatenate([pieces[j][...], pieces[len(members) + j][...]], axis=1)
        for j in range(len(members))
    ]
    rights = [weight_rows(w_ref, group, k, slice(None)) for k in members]
    for tile in range(tiles.shape[0]):
        rows = slice(tile * height, (tile + 1) * height)
        total = total_ref[rows, :]
        for left, right in zip(lefts, rights):
            total += dot(left[rows], right)
        tiles[tile] = total.astype(jnp.bfloat16)
        part = out_ref.at[pl.ds(tile * height, height)]
        copies.append(pltpu.make_async_copy(tiles.at[tile], part, sems.at[tile]))
        copies[-1].start()
    for copy in copies:
        copy.wait()


def early_kernel(group, members, *refs):
    pieces = refs[: 2 * len(members)]
    w_ref, total_ref = refs[2 * len(members) :]
    total = None
    for j, k in enumerate(members):
        left = jnp.concatenate([pieces[j][...], pieces[len(members) + j][...]], axis=1)
        term = dot(left, weight_rows(w_ref, group, k, slice(None)))
        total = term if total is None else total + term
    total_ref[...] = total


def project_early(group, members, own, other, w_out):
    return pl.pallas_call(
        functools.partial(early_kernel, group, members),
        out_shape=jax.ShapeDtypeStruct((own[0].shape[0], w_out.shape[1]), jnp.float32),
        in_specs=[pl.BlockSpec(memory_space=pltpu.VMEM)] * (2 * len(members) + 1),
        out_specs=pl.BlockSpec(memory_space=pltpu.VMEM),
        compiler_params=pltpu.CompilerParams(vmem_limit_bytes=VMEM_LIMIT),
        cost_estimate=pl.CostEstimate(flops=10**6, bytes_accessed=10**6, transcendentals=0),
    )(*[x[k] for x in (own, other) for k in members], w_out)


def project(group, members, own, other, w_out, total):
    rows, width = own[0].shape[0], w_out.shape[1]
    tile = 128
    return pl.pallas_call(
        functools.partial(project_kernel, group, members),
        out_shape=jax.ShapeDtypeStruct((rows, width), jnp.bfloat16),
        in_specs=[pl.BlockSpec(memory_space=pltpu.VMEM)] * (2 * len(members) + 2),
        out_specs=pl.BlockSpec(memory_space=pl.ANY),
        scratch_shapes=[
            pltpu.VMEM((rows // tile, tile, width), jnp.bfloat16),
            pltpu.SemaphoreType.DMA((rows // tile,)),
        ],
        compiler_params=pltpu.CompilerParams(vmem_limit_bytes=VMEM_LIMIT),
        cost_estimate=pl.CostEstimate(flops=10**9, bytes_accessed=10**6, transcendentals=0),
    )(*[x[k] for x in (own, other) for k in members], w_out, total)


def per_device(queries, keys, values, w_out):
    rows = queries.shape[0]
    shards = lax.axis_size("sp")
    group = -(-(SIDE_KEY_COUNT * FAR_DILATION) // rows)
    groups = shards // group

    def inside(value, k):
        return lax.ppermute(value, "sp", [(s, s ^ k) for s in range(shards)])

    def across(value, parity):
        pairs = []
        for s in range(shards):
            mine = s // group
            beside = mine + 1 if mine % 2 == parity else mine - 1
            for t in range(2):
                if 0 <= beside < groups:
                    pairs.append((2 * s + t, 2 * (s + (beside - mine) * group) + t))
                else:
                    pairs.append((2 * s + t, 2 * s + 1 - t))
        return lax.ppermute(value, ("sp", "tp"), pairs)

    def other_core(value):
        return lax.ppermute(value, "tp", [(0, 1), (1, 0)])

    kv, q = spread(group, keys, values, queries)
    own = [kv[0]] + [inside(kv[k], k) for k in range(1, group)]
    q = {k: inside(q[k], k) if k else q[k] for k in q}
    parcels = [pile([own[k] for k in members]) for members in PARCELS]
    even = [across(parcel, 0) for parcel in parcels]
    odd = [across(parcel, 1) for parcel in parcels]
    far_own, middle_own, near_own, far_halo, touch_halo, ends, natural = masks(group, groups, rows)
    found = attend_local(group, q, own, (far_own, middle_own, near_own, ends))
    out = attend_halo(group, found, even, odd, (far_halo, touch_halo, ends, natural))
    out = [out[0]] + [inside(out[k], k) for k in range(1, group)]
    swapped = [other_core(piece) for piece in out]
    total = project_early(group, EARLY, out, swapped, w_out)
    late = [k for k in range(group) if k not in EARLY]
    return project(group, late, out, swapped, w_out, total)


PARCELS = ((0,), (1, 2), (3,))
MERGED = (3,)
EARLY = (0, 1)


def solution(mesh):
    in_specs = (P("sp", "tp"), P("sp", "tp"), P("sp", "tp"), P(None, "tp"))
    out_specs = P("sp", "tp")
    return jax.shard_map(
        per_device, mesh=mesh, in_specs=in_specs, out_specs=out_specs, check_vma=False
    )
```
